512 devices in a mesh: grp: 2 (over y), kv: 16 (over z), tp: 16 (over x, core).
Axes of the slice: x: 8, y: 2, z: 16, core: 2. Of those that a mesh axis runs over, the one named last changes fastest.
The devices are a block of a 8x16x16 slice.
Arguments:
- tokens: bfloat16 [256, 4096], P('grp', ('kv', 'tp')), parts along dimension 0, may hold values from -8 to 8
- norm_gain: bfloat16 [4096], P('kv'), may hold values from 0.099609375 to 1.8984375
- w_query: bfloat16 [4096, 1024], P('kv', 'tp'), may hold values from -0.09375 to 0.09375
- w_key: bfloat16 [4096, 1024], P('kv', 'tp'), may hold values from -0.09375 to 0.09375
- w_value: bfloat16 [4096, 2048], P('kv', 'tp'), may hold values from -0.09375 to 0.09375
- w_ogate: bfloat16 [4096, 2048], P('kv', 'tp'), may hold values from -0.09375 to 0.09375
- w_igate: bfloat16 [4096, 16], P('kv', 'tp'), may hold values from -0.09375 to 0.09375
- w_fgate: bfloat16 [4096, 16], P('kv', 'tp'), may hold values from -0.09375 to 0.09375
- igate_bias: float32 [16], P('tp'), may hold values from -1 to 1
- fgate_bias: float32 [16], P('tp'), may hold values from -1 to 4
- state_c: float32 [256, 16, 64, 128], P(('grp', 'kv'), 'tp'), parts along dimension 0, may hold values from -1.5 to 1.5
- state_n: float32 [256, 16, 64], P(('grp', 'kv'), 'tp'), parts along dimension 0, may hold values from -1.5 to 1.5
- state_m: float32 [256, 16], P(('grp', 'kv'), 'tp'), parts along dimension 0, may hold values from -3 to 1
- head_gain: bfloat16 [16, 128], P('tp'), may hold values from 0.099609375 to 1.8984375
- w_out: bfloat16 [2048, 4096], P('tp', 'kv'), may hold values from -0.125 to 0.125
- ffn_gain: bfloat16 [4096], P('kv'), may hold values from 0.099609375 to 1.8984375
- w_gate: bfloat16 [4096, 11008], P('kv', 'tp'), may hold values from -0.09375 to 0.09375
- w_up: bfloat16 [4096, 11008], P('kv', 'tp'), may hold values from -0.09375 to 0.09375
- w_down: bfloat16 [11008, 4096], P('tp', 'kv'), may hold values from -0.0546875 to 0.0546875
Outputs:
- out_tokens: bfloat16 [256, 4096], P('grp', ('kv', 'tp')), parts along dimension 0
- new_c: float32 [256, 16, 64, 128], P(('grp', 'kv'), 'tp'), parts along dimension 0
- new_n: float32 [256, 16, 64], P(('grp', 'kv'), 'tp'), parts along dimension 0
- new_m: float32 [256, 16], P(('grp', 'kv'), 'tp'), parts along dimension 0
The draws below stay inside these ranges and needn't reach their ends.
There are 2 independent parts, one for each index of `grp`. The reference program is written for one: setup_inputs(seed, part) draws one part's arguments, and reference() takes and returns one part's arrays. A program takes and returns all parts, laid end to end along the dimension named above; an argument that names none is the same for every part. Nothing has to cross between parts.
All inputs are finite; a program needn't handle non-finite values.
Results may differ from the reference program's by a relative error of at most 0.017.
Values may be sent and summed in bfloat16 or wider, within the bound.
No kernel may reach another device: no remote copies, remote signals or barrier semaphores. Data moves between devices by JAX's collectives and lax.ppermute only.
A program may use at most 64 MiB of HBM per device.

```python
import math
import jax
import jax.numpy as jnp
from jax import lax

D = 4096
HEADS = 16
DK = 64
DV = 128
FF = 11008
SEQS = 128


def draw_tokens(key, part):
    first, second, third = jax.random.split(jax.random.fold_in(key, 11), 3)
    position = jnp.arange(D, dtype=jnp.float32) / D
    column_scale = jnp.exp((position - 0.5) * math.log(3.0)) * jnp.exp(jax.random.uniform(second, (D,), jnp.float32, -0.35, 0.35))
    row_scale = jnp.exp(jax.random.uniform(third, (SEQS, 1), jnp.float32, 0.0, math.log(10.0))) / 3.0
    base = jax.random.normal(first, (SEQS, D), jnp.float32)
    return jnp.clip(base * row_scale * column_scale, -8.0, 8.0).astype(jnp.bfloat16)


def level_of(key, dims, pieces, low, high):
    loudness = 1.0
    for axis_at, parts in pieces:
        steps = jax.random.uniform(jax.random.fold_in(jax.random.fold_in(key, 6), axis_at), (parts,), jnp.float32, low / len(pieces), high / len(pieces))
        loudness = loudness * jnp.repeat(jnp.exp(steps), dims[axis_at] // parts).reshape((-1,) + (1,) * (len(dims) - 1 - axis_at))
    return loudness


def normal_values(key, dims, deviation, most, cuts=(), kind=jnp.bfloat16):
    loudness = level_of(key, dims, cuts, -0.22, 0.18) if cuts else 1.0
    values = jax.random.normal(key, dims, jnp.float32) * deviation * loudness
    return jnp.minimum(jnp.maximum(values, -most), most).astype(kind)


def setup_inputs(seed: int = 0, part: int = 0) -> dict:
    key_list = jax.random.split(jax.random.key(seed), 20)
    own_keys = jax.random.split(jax.random.fold_in(key_list[19], part), 20)
    tokens = draw_tokens(jax.random.fold_in(jax.random.fold_in(key_list[19], part), 71), part)
    norm_gain = jnp.clip(1.0 + 0.18 * jax.random.normal(key_list[1], (D,), jnp.float32), 0.099609375, 1.8984375).astype(jnp.bfloat16)
    w_query = normal_values(key_list[2], (D, HEADS * DK), D ** -0.5, 0.09375, ((0, 16), (1, 16)))
    w_key = normal_values(key_list[3], (D, HEADS * DK), D ** -0.5, 0.09375, ((0, 16), (1, 16)))
    w_value = normal_values(key_list[4], (D, HEADS * DV), D ** -0.5, 0.09375, ((0, 16), (1, 16)))
    w_ogate = normal_values(key_list[5], (D, HEADS * DV), D ** -0.5, 0.09375, ((0, 16), (1, 16)))
    w_igate = normal_values(key_list[6], (D, HEADS), D ** -0.5, 0.09375, ((0, 16), (1, 16)))
    w_fgate = normal_values(key_list[7], (D, HEADS), D ** -0.5, 0.09375, ((0, 16), (1, 16)))
    igate_bias = jnp.clip(jax.random.uniform(key_list[8], (HEADS,), jnp.float32, -1.0, 1.0) * level_of(key_list[8], (HEADS,), ((0, 16),), -0.4, 0.0), -1.0, 1.0)
    fgate_bias = jnp.clip(-1.0 + 5.0 * jax.random.uniform(key_list[9], (HEADS,), jnp.float32) ** level_of(key_list[9], (HEADS,), ((0, 16),), -0.2, 0.2), -1.0, 4.0)
    state_c = normal_values(own_keys[10], (SEQS, HEADS, DK, DV), 0.25, 1.5, ((0, 16), (1, 16)), jnp.float32)
    state_n = normal_values(own_keys[11], (SEQS, HEADS, DK), 0.25, 1.5, ((0, 16), (1, 16)), jnp.float32)
    state_m = jnp.clip(-3.0 + 4.0 * jax.random.uniform(own_keys[12], (SEQS, HEADS), jnp.float32) ** level_of(own_keys[12], (SEQS, HEADS), ((0, 16), (1, 16)), -0.2, 0.2), -3.0, 1.0)
    head_gain = jnp.clip(1.0 + 0.18 * jax.random.normal(key_list[13], (HEADS, DV), jnp.float32), 0.099609375, 1.8984375).astype(jnp.bfloat16)
    w_out = normal_values(key_list[14], (HEADS * DV, D), (HEADS * DV) ** -0.5, 0.125, ((0, 16), (1, 16)))
    ffn_gain = jnp.clip(1.0 + 0.18 * jax.random.normal(key_list[15], (D,), jnp.float32), 0.099609375, 1.8984375).astype(jnp.bfloat16)
    w_gate = normal_values(key_list[16], (D, FF), D ** -0.5, 0.09375, ((0, 16), (1, 16)))
    w_up = normal_values(key_list[17], (D, FF), D ** -0.5, 0.09375, ((0, 16), (1, 16)))
    w_down = normal_values(key_list[18], (FF, D), FF ** -0.5, 0.0546875, ((0, 16), (1, 16)))
    return dict(tokens=tokens, norm_gain=norm_gain, w_query=w_query, w_key=w_key, w_value=w_value, w_ogate=w_ogate, w_igate=w_igate, w_fgate=w_fgate, igate_bias=igate_bias, fgate_bias=fgate_bias, state_c=state_c, state_n=state_n, state_m=state_m, head_gain=head_gain, w_out=w_out, ffn_gain=ffn_gain, w_gate=w_gate, w_up=w_up, w_down=w_down)


norm_eps = 1e-06
igate_cap = 1.5

def cell_update(query, key_vec, value_vec, igate, fgate, state_c, state_n, state_m):
    carried = jax.nn.log_sigmoid(fgate) + state_m
    new_m = jnp.maximum(carried, igate)
    keep_weight = jnp.exp(carried - new_m)
    write_weight = jnp.exp(igate - new_m)
    new_c = keep_weight[..., None, None] * state_c + write_weight[..., None, None] * key_vec[..., :, None] * value_vec[..., None, :]
    new_n = keep_weight[..., None] * state_n + write_weight[..., None] * key_vec
    numerator = jnp.einsum('bhd,bhde->bhe', query, new_c, precision=lax.Precision.HIGHEST)
    denominator = lax.optimization_barrier(jnp.sum(query * new_n, axis=-1))
    head_out = numerator / jnp.maximum(jnp.abs(denominator), jnp.exp(-new_m))[..., None]
    return (new_c, new_n, new_m, head_out)

def reference(tokens, norm_gain, w_query, w_key, w_value, w_ogate, w_igate, w_fgate, igate_bias, fgate_bias, state_c, state_n, state_m, head_gain, w_out, ffn_gain, w_gate, w_up, w_down):
    token_vals = tokens.astype(jnp.float32)
    row_scale = lax.rsqrt(lax.optimization_barrier(jnp.mean(token_vals * token_vals, axis=1, keepdims=True)) + norm_eps)
    normed = (token_vals * norm_gain.astype(jnp.float32)).astype(jnp.bfloat16)

    def project(weight):
        return row_scale * jnp.dot(normed, weight, preferred_element_type=jnp.float32)
    query = project(w_query).reshape(SEQS, HEADS, DK)
    key_vec = project(w_key).reshape(SEQS, HEADS, DK) * DK ** (-0.5)
    value_vec = project(w_value).reshape(SEQS, HEADS, DV)
    ogate = project(w_ogate).reshape(SEQS, HEADS, DV)
    igate = igate_cap * jnp.tanh((project(w_igate) + igate_bias) / igate_cap)
    fgate = project(w_fgate) + fgate_bias
    new_c, new_n, new_m, head_out = cell_update(query, key_vec, value_vec, igate, fgate, state_c, state_n, state_m)
    merged = (head_out * head_gain.astype(jnp.float32) * jax.nn.sigmoid(ogate)).reshape(SEQS, HEADS * DV).astype(jnp.bfloat16)
    attn_out = jnp.dot(merged, w_out, preferred_element_type=jnp.float32)
    middle = (token_vals + attn_out).astype(jnp.bfloat16)
    middle_vals = middle.astype(jnp.float32)
    ffn_scale = lax.rsqrt(lax.optimization_barrier(jnp.mean(middle_vals * middle_vals, axis=1, keepdims=True)) + norm_eps)
    normed_two = (middle_vals * ffn_gain.astype(jnp.float32)).astype(jnp.bfloat16)
    gate_sum = ffn_scale * jnp.dot(normed_two, w_gate, preferred_element_type=jnp.float32)
    up_sum = ffn_scale * jnp.dot(normed_two, w_up, preferred_element_type=jnp.float32)
    hidden = (jax.nn.silu(gate_sum) * up_sum).astype(jnp.bfloat16)
    out_tokens = (middle_vals + jnp.dot(hidden, w_down, preferred_element_type=jnp.float32)).astype(jnp.bfloat16)
    return (out_tokens, new_c, new_n, new_m)
```

```python
import math

import jax
import jax.numpy as jnp
from jax import lax
from jax.sharding import PartitionSpec as P

D = 4096
DK = 64
DV = 128


norm_eps = 1e-06
igate_cap = 1.5


def split_up(value, dim, count):
    before, after = (value.shape[:dim], value.shape[dim + 1 :])
    return jnp.moveaxis(value.reshape(*before, count, -1, *after), dim, 0)


def side_by_side(arrays, axis, dim, along):
    columns = [a.reshape(*a.shape[:along], -1) for a in arrays]
    both = jnp.concatenate(columns, axis=along).astype(jnp.bfloat16)
    out, at, finished = (sum_at_owner(both, axis, dim), 0, [])
    for a, column in zip(arrays, columns):
        section = out[..., at : at + column.shape[along]]
        finished.append(section.reshape(*section.shape[:along], *a.shape[along:]))
        at += column.shape[along]
    return tuple(finished)


def in_order(blocks, dim):
    lengths = list(blocks.shape[1:])
    lengths[dim] *= blocks.shape[0]
    return jnp.moveaxis(blocks, 0, dim).reshape(lengths)


def sent_to_all(value, axis):
    count = lax.axis_size(axis)
    return lax.all_to_all(
        jnp.broadcast_to(value[None], (count, *value.shape)), axis, 0, 0, tiled=True
    )


def gathered_copies(value, axis, dim):
    return in_order(sent_to_all(value, axis), dim)


def sum_at_owner(value, axis, dim):
    blocks = split_up(value, dim, lax.axis_size(axis))
    arrived = lax.all_to_all(blocks, axis, split_axis=0, concat_axis=0, tiled=True)
    return arrived.astype(jnp.float32).sum(axis=0)


def side_by_side_2(arrays, axis, dim, along):
    widths = [math.prod(a.shape[along:]) for a in arrays]
    both = jnp.concatenate(
        [a.reshape(*a.shape[:along], w) for a, w in zip(arrays, widths)], axis=along
    )
    out = sum_at_owner(both, axis, dim)
    blocks = jnp.split(out, [sum(widths[:k]) for k in range(1, len(widths))], axis=along)
    return tuple((b.reshape(*out.shape[:along], *a.shape[along:]) for a, b in zip(arrays, blocks)))


def cell_update(query, key_vec, value_vec, igate, fgate, state_c, state_n, state_m):
    carried = jax.nn.log_sigmoid(fgate) + state_m
    new_m = jnp.maximum(carried, igate)
    keep_weight = jnp.exp(carried - new_m)
    write_weight = jnp.exp(igate - new_m)
    new_c = (
        keep_weight[..., None, None] * state_c
        + write_weight[..., None, None] * key_vec[..., :, None] * value_vec[..., None, :]
    )
    new_n = keep_weight[..., None] * state_n + write_weight[..., None] * key_vec
    numerator = jnp.einsum("bhd,bhde->bhe", query, new_c, precision=lax.Precision.HIGHEST)
    denominator = jnp.sum(query * new_n, axis=-1)
    head_out = numerator / jnp.maximum(jnp.abs(denominator), jnp.exp(-new_m))[..., None]
    return (new_c, new_n, new_m, head_out)


def body(
    tokens,
    norm_gain,
    w_query,
    w_key,
    w_value,
    w_ogate,
    w_igate,
    w_fgate,
    igate_bias,
    fgate_bias,
    state_c,
    state_n,
    state_m,
    head_gain,
    w_out,
    ffn_gain,
    w_gate,
    w_up,
    w_down,
):
    seq_rows = state_c.shape[0]
    heads_here = state_c.shape[1]
    token_cols = gathered_copies(tokens, "tp", 1)
    token_vals = token_cols.astype(jnp.float32)
    normed = (token_vals * norm_gain.astype(jnp.float32)).astype(jnp.bfloat16)
    squares = jnp.sum(token_vals * token_vals, axis=1)
    part_query = jnp.dot(normed, w_query, preferred_element_type=jnp.float32)
    part_key = jnp.dot(normed, w_key, preferred_element_type=jnp.float32)
    part_value = jnp.dot(normed, w_value, preferred_element_type=jnp.float32)
    part_ogate = jnp.dot(normed, w_ogate, preferred_element_type=jnp.float32)
    part_igate = jnp.dot(normed, w_igate, preferred_element_type=jnp.float32)
    part_fgate = jnp.dot(normed, w_fgate, preferred_element_type=jnp.float32)
    sum_query, sum_key, sum_value, sum_ogate, sum_igate, sum_fgate, sum_squares = side_by_side(
        (part_query, part_key, part_value, part_ogate, part_igate, part_fgate, squares), "kv", 0, 1
    )
    row_scale = lax.rsqrt(sum_squares / D + norm_eps)[:, None]
    query = (row_scale * sum_query).reshape(seq_rows, heads_here, DK)
    key_vec = (row_scale * sum_key).reshape(seq_rows, heads_here, DK) * DK ** (-0.5)
    value_vec = (row_scale * sum_value).reshape(seq_rows, heads_here, DV)
    ogate = (row_scale * sum_ogate).reshape(seq_rows, heads_here, DV)
    igate = igate_cap * jnp.tanh((row_scale * sum_igate + igate_bias) / igate_cap)
    fgate = row_scale * sum_fgate + fgate_bias
    new_c, new_n, new_m, head_out = cell_update(
        query, key_vec, value_vec, igate, fgate, state_c, state_n, state_m
    )
    merged = (
        (head_out * head_gain.astype(jnp.float32) * jax.nn.sigmoid(ogate))
        .reshape(seq_rows, heads_here * DV)
        .astype(jnp.bfloat16)
    )
    attn_part = jnp.dot(gathered_copies(merged, "kv", 0), w_out, preferred_element_type=jnp.float32)
    attn_out = sum_at_owner(attn_part.astype(jnp.bfloat16), "tp", 1)
    middle = (tokens.astype(jnp.float32) + attn_out).astype(jnp.bfloat16)
    middle_cols = gathered_copies(middle, "tp", 1)
    middle_vals = middle_cols.astype(jnp.float32)
    normed_two = (middle_vals * ffn_gain.astype(jnp.float32)).astype(jnp.bfloat16)
    squares_two = jnp.sum(middle_vals * middle_vals, axis=1)
    gate_part = jnp.dot(normed_two, w_gate, preferred_element_type=jnp.float32)
    up_part = jnp.dot(normed_two, w_up, preferred_element_type=jnp.float32)
    gate_sum, up_sum, total_two = side_by_side_2(
        (
            gate_part.astype(jnp.bfloat16),
            up_part.astype(jnp.bfloat16),
            squares_two.astype(jnp.bfloat16),
        ),
        "kv",
        0,
        1,
    )
    ffn_scale = lax.rsqrt(total_two / D + norm_eps)[:, None]
    hidden = (jax.nn.silu(ffn_scale * gate_sum) * (ffn_scale * up_sum)).astype(jnp.bfloat16)
    down_part = jnp.dot(
        gathered_copies(hidden, "kv", 0), w_down, preferred_element_type=jnp.float32
    )
    down_out = sum_at_owner(down_part.astype(jnp.bfloat16), "tp", 1)
    out_tokens = (middle.astype(jnp.float32) + down_out).astype(jnp.bfloat16)
    return (out_tokens, new_c, new_n, new_m)


def solution(mesh):
    placed = (
        P("grp", ("kv", "tp")),
        P("kv"),
        P("kv", "tp"),
        P("kv", "tp"),
        P("kv", "tp"),
        P("kv", "tp"),
        P("kv", "tp"),
        P("kv", "tp"),
        P("tp"),
        P("tp"),
        P(("grp", "kv"), "tp", None, None),
        P(("grp", "kv"), "tp", None),
        P(("grp", "kv"), "tp"),
        P("tp", None),
        P("tp", "kv"),
        P("kv"),
        P("kv", "tp"),
        P("kv", "tp"),
        P("tp", "kv"),
    )
    return jax.shard_map(
        body,
        mesh=mesh,
        in_specs=placed,
        out_specs=(
            P("grp", ("kv", "tp")),
            P(("grp", "kv"), "tp", None, None),
            P(("grp", "kv"), "tp", None),
            P(("grp", "kv"), "tp"),
        ),
        check_vma=False,
    )
```

```python
import jax
import jax.numpy as jnp
from jax import lax
from jax.experimental import pallas as pl
from jax.experimental.pallas import tpu as pltpu
from jax.sharding import PartitionSpec as P

D = 4096
DK = 64
DV = 128
LANES = 128


norm_eps = 1e-06
igate_cap = 1.5

VMEM = pl.BlockSpec(memory_space=pltpu.VMEM)
ANY = pl.BlockSpec(memory_space=pl.ANY)
HBM = pl.BlockSpec(memory_space=pltpu.HBM)
SMALL = pltpu.CompilerParams(vmem_limit_bytes=8 * 2**20)


def exchanged(blocks, axis):
    return lax.all_to_all(blocks, axis, split_axis=0, concat_axis=0, tiled=True)


def spread_kernel(value_ref, out_ref):
    value = value_ref[...]
    for copy in range(out_ref.shape[0]):
        out_ref[copy] = value


def spread(value, count):
    return pl.pallas_call(
        spread_kernel,
        out_shape=jax.ShapeDtypeStruct((count, *value.shape), value.dtype),
        in_specs=[VMEM],
        out_specs=VMEM,
        compiler_params=SMALL,
        name="spread",
    )(value)


def project_kernel(
    x_ref, gain_ref, query_ref, key_ref, value_ref, ogate_ref, igate_ref, fgate_ref,
    ibias_ref, fbias_ref, out_ref, bias_ref, qk, val, og, biases, sems,
):
    copies = [
        pltpu.make_async_copy(query_ref, qk.at[pl.ds(0, DK)], sems.at[0]),
        pltpu.make_async_copy(key_ref, qk.at[pl.ds(DK, DK)], sems.at[1]),
        pltpu.make_async_copy(value_ref, val, sems.at[2]),
        pltpu.make_async_copy(ogate_ref, og, sems.at[3]),
        pltpu.make_async_copy(ibias_ref, biases.at[0], sems.at[4]),
        pltpu.make_async_copy(fbias_ref, biases.at[1], sems.at[5]),
    ]
    for copy in copies:
        copy.start()
    x = x_ref[...].astype(jnp.float32).T
    normed = (x * gain_ref[...].astype(jnp.float32)[None, :]).astype(jnp.bfloat16)
    wide = normed.astype(jnp.float32)
    squares = jnp.sum(x * x, axis=1, keepdims=True)
    igate = jnp.sum(wide * igate_ref[...].astype(jnp.float32), axis=1, keepdims=True)
    fgate = jnp.sum(wide * fgate_ref[...].astype(jnp.float32), axis=1, keepdims=True)
    lane = lax.broadcasted_iota(jnp.int32, (x.shape[0], LANES), 1)
    tail = jnp.where(lane == 0, igate, jnp.where(lane == 1, fgate, jnp.where(lane == 2, squares, 0.0)))
    out_ref[:, 3 * LANES :] = tail.astype(out_ref.dtype)
    copies[0].wait()
    copies[1].wait()
    both = lax.dot_general(
        normed, qk[...], (((1,), (1,)), ((), ())), preferred_element_type=jnp.float32
    )
    out_ref[:, :LANES] = both.astype(out_ref.dtype)
    copies[2].wait()
    out_ref[:, LANES : 2 * LANES] = jnp.dot(
        normed, val[...], preferred_element_type=jnp.float32
    ).astype(out_ref.dtype)
    copies[3].wait()
    out_ref[:, 2 * LANES : 3 * LANES] = jnp.dot(
        normed, og[...], preferred_element_type=jnp.float32
    ).astype(out_ref.dtype)
    copies[4].wait()
    copies[5].wait()
    row = lax.broadcasted_iota(jnp.int32, bias_ref.shape, 0)
    bias_ref[...] = jnp.where(row == 0, biases[0, 0], biases[1, 0])


def project(
    x, gain, w_query, w_key, w_value, w_ogate, w_igate, w_fgate, igate_bias, fgate_bias
):
    rows, seqs = x.shape
    return pl.pallas_call(
        project_kernel,
        out_shape=(
            jax.ShapeDtypeStruct((seqs, 4 * LANES), jnp.bfloat16),
            jax.ShapeDtypeStruct((8, LANES), jnp.float32),
        ),
        in_specs=[VMEM, VMEM, ANY, ANY, ANY, ANY, VMEM, VMEM, HBM, HBM],
        out_specs=(VMEM, VMEM),
        scratch_shapes=[
            pltpu.VMEM((2 * DK, rows), jnp.bfloat16),
            pltpu.VMEM((rows, DV), jnp.bfloat16),
            pltpu.VMEM((rows, DV), jnp.bfloat16),
            pltpu.SMEM((2, 1), jnp.float32),
            pltpu.SemaphoreType.DMA((6,)),
        ],
        compiler_params=SMALL,
        name="project",
    )(x, gain, w_query.T, w_key.T, w_value, w_ogate, w_igate.T, w_fgate.T,
      igate_bias, fgate_bias)


def cell_kernel(
    parts_ref, bias_ref, c_ref, n_ref, m_ref, gain_ref,
    new_c_out, new_n_ref, new_m_ref, out_ref, new_c_ref, sem,
):
    total = parts_ref[0].astype(jnp.float32)
    for k in range(1, parts_ref.shape[0]):
        total += parts_ref[k].astype(jnp.float32)
    seqs = total.shape[0]
    tail = total[:, 3 * LANES :]
    row_scale = lax.rsqrt(tail[:, 2:3] / D + norm_eps)
    igate = igate_cap * jnp.tanh((row_scale * tail[:, 0:1] + bias_ref[0:1, 0:1]) / igate_cap)
    fgate = row_scale * tail[:, 1:2] + bias_ref[1:2, 0:1]
    diagonal = lax.broadcasted_iota(jnp.int32, (seqs, seqs), 0) == lax.broadcasted_iota(
        jnp.int32, (seqs, seqs), 1
    )
    state_m = jnp.sum(jnp.where(diagonal, m_ref[...], 0.0), axis=1, keepdims=True)
    log_keep = jnp.minimum(fgate, 0.0) - jnp.log1p(jnp.exp(-jnp.abs(fgate)))
    carried = log_keep + state_m
    new_m = jnp.maximum(carried, igate)
    keep = jnp.exp(carried - new_m)
    write = jnp.exp(igate - new_m)
    new_m_ref[...] = jnp.sum(jnp.where(diagonal, new_m, 0.0), axis=0, keepdims=True)
    lane = lax.broadcasted_iota(jnp.int32, (seqs, LANES), 1)
    first = total[:, :LANES]
    query_key = row_scale * jnp.where(lane < DK, first, first * DK ** (-0.5))
    query = query_key[:, :DK]
    key_vec = query_key[:, DK:]
    value_vec = row_scale * total[:, LANES : 2 * LANES]
    ogate = row_scale * total[:, 2 * LANES : 3 * LANES]
    new_n = keep * n_ref[...] + write * key_vec
    new_n_ref[...] = new_n
    denominator = jnp.maximum(
        jnp.abs(jnp.sum(query * new_n, axis=1, keepdims=True)), jnp.exp(-new_m)
    )
    columns = jnp.where(lane < DK, query_key, write * query_key).T
    for b in range(seqs):
        key_b = columns[DK:, b : b + 1]
        new_c_ref[b] = keep[b : b + 1, :] * c_ref[b] + key_b * value_vec[b : b + 1, :]
    copy_out = pltpu.make_async_copy(new_c_ref, new_c_out, sem)
    copy_out.start()
    rows = []
    for b in range(seqs):
        query_b = columns[:DK, b : b + 1]
        rows.append(jnp.sum(query_b * new_c_ref[b], axis=0, keepdims=True))
    head_out = jnp.concatenate(rows, axis=0) / denominator
    merged = head_out * gain_ref[...].astype(jnp.float32) / (1.0 + jnp.exp(-ogate))
    merged = merged.astype(out_ref.dtype)
    for copy in range(out_ref.shape[0]):
        out_ref[copy] = merged
    copy_out.wait()


def cell(parts, biases, state_c, state_n, state_m, head_gain):
    count, seqs, _ = parts.shape
    new_c, new_n, new_m, out = pl.pallas_call(
        cell_kernel,
        out_shape=(
            jax.ShapeDtypeStruct((seqs, DK, DV), jnp.float32),
            jax.ShapeDtypeStruct((seqs, DK), jnp.float32),
            jax.ShapeDtypeStruct((1, seqs), jnp.float32),
            jax.ShapeDtypeStruct((count, seqs, DV), jnp.bfloat16),
        ),
        in_specs=[VMEM] * 6,
        out_specs=(ANY, VMEM, VMEM, VMEM),
        scratch_shapes=[
            pltpu.VMEM((seqs, DK, DV), jnp.float32),
            pltpu.SemaphoreType.DMA,
        ],
        compiler_params=SMALL,
        name="cell",
    )(
        parts, biases, state_c.reshape(seqs, DK, DV),
        state_n.reshape(seqs, DK), state_m.T, head_gain,
    )
    return new_c.reshape(state_c.shape), new_n.reshape(state_n.shape), new_m.T, out


def residual_kernel(parts_ref, tokens_ref, out_ref):
    total = parts_ref[0].astype(jnp.float32)
    for k in range(1, parts_ref.shape[0]):
        total += parts_ref[k].astype(jnp.float32)
    middle = (tokens_ref[0].astype(jnp.float32) + total).astype(out_ref.dtype)
    for copy in range(out_ref.shape[0]):
        out_ref[copy] = middle


def residual(parts, copies):
    return pl.pallas_call(
        residual_kernel,
        out_shape=jax.ShapeDtypeStruct(copies.shape, copies.dtype),
        in_specs=[VMEM, VMEM],
        out_specs=VMEM,
        compiler_params=SMALL,
        name="residual",
    )(parts, copies)


def widen_kernel(x_ref, gain_ref, gate_ref, up_ref, out_ref, weights, sems):
    units = gate_ref.shape[0]
    cols = out_ref.shape[1]
    gate_copy = pltpu.make_async_copy(gate_ref, weights.at[pl.ds(0, units)], sems.at[0])
    up_copy = pltpu.make_async_copy(up_ref, weights.at[pl.ds(units, units)], sems.at[1])
    gate_copy.start()
    up_copy.start()
    weights[2 * units :, :] = jnp.zeros((cols - 2 * units, weights.shape[1]), weights.dtype)
    x = x_ref[...].astype(jnp.float32).T
    normed = (x * gain_ref[...].astype(jnp.float32)[None, :]).astype(jnp.bfloat16)
    squares = jnp.sum(x * x, axis=1, keepdims=True)
    gate_copy.wait()
    start = units // LANES * LANES

    def product(at, size):
        return lax.dot_general(
            normed, weights[at : at + size, :], (((1,), (1,)), ((), ())),
            preferred_element_type=jnp.float32,
        )

    out_ref[:, :start] = product(0, start).astype(out_ref.dtype)
    up_copy.wait()
    last = cols - LANES
    out_ref[:, start:last] = product(start, last - start).astype(out_ref.dtype)
    lane = lax.broadcasted_iota(jnp.int32, (x.shape[0], LANES), 1)
    tail = jnp.where(lane == 2 * units - last, squares, product(last, LANES))
    out_ref[:, last:] = tail.astype(out_ref.dtype)


def widen(x, gain, w_gate, w_up):
    rows, seqs = x.shape
    cols = (2 * w_gate.shape[1] // LANES + 1) * LANES
    return pl.pallas_call(
        widen_kernel,
        out_shape=jax.ShapeDtypeStruct((seqs, cols), jnp.bfloat16),
        in_specs=[VMEM, VMEM, ANY, ANY],
        out_specs=VMEM,
        scratch_shapes=[
            pltpu.VMEM((cols, rows), jnp.bfloat16),
            pltpu.SemaphoreType.DMA((2,)),
        ],
        compiler_params=SMALL,
        name="widen",
    )(x, gain, w_gate.T, w_up.T)


def body(
    tokens,
    norm_gain,
    w_query,
    w_key,
    w_value,
    w_ogate,
    w_igate,
    w_fgate,
    igate_bias,
    fgate_bias,
    state_c,
    state_n,
    state_m,
    head_gain,
    w_out,
    ffn_gain,
    w_gate,
    w_up,
    w_down,
):
    n_kv, n_tp = lax.axis_size("kv"), lax.axis_size("tp")
    seqs, feats = tokens.shape
    units = w_gate.shape[1]
    rows = n_tp * feats
    own_seqs = seqs // n_kv

    token_copies = spread(tokens.T, n_tp)
    token_rows = exchanged(token_copies, "tp").reshape(rows, seqs)
    parts, biases = project(
        token_rows, norm_gain, w_query, w_key, w_value, w_ogate, w_igate, w_fgate,
        igate_bias, fgate_bias,
    )
    arrived = exchanged(parts.reshape(n_kv, own_seqs, -1), "kv")
    new_c, new_n, new_m, merged = cell(
        arrived, biases, state_c, state_n, state_m, head_gain
    )
    merged_all = exchanged(merged, "kv").reshape(seqs, -1)
    attn_part = jnp.dot(merged_all, w_out, preferred_element_type=jnp.float32)
    attn_part = attn_part.astype(jnp.bfloat16).T.reshape(n_tp, feats, seqs)
    middle_copies = residual(exchanged(attn_part, "tp"), token_copies)
    middle_rows = exchanged(middle_copies, "tp").reshape(rows, seqs)
    wide = widen(middle_rows, ffn_gain, w_gate, w_up)
    sums = exchanged(wide.reshape(n_kv, own_seqs, -1), "kv").astype(jnp.float32).sum(axis=0)
    gate_sum, up_sum, total = sums[:, :units], sums[:, units : 2 * units], sums[:, 2 * units]
    ffn_scale = lax.rsqrt(total / D + norm_eps)[:, None]
    hidden = (jax.nn.silu(ffn_scale * gate_sum) * (ffn_scale * up_sum)).astype(jnp.bfloat16)
    hidden_all = exchanged(
        jnp.broadcast_to(hidden[None], (n_kv, *hidden.shape)), "kv"
    ).reshape(seqs, units)
    down_part = jnp.dot(hidden_all, w_down, preferred_element_type=jnp.float32)
    down_part = down_part.astype(jnp.bfloat16).T.reshape(n_tp, feats, seqs)
    down_out = exchanged(down_part, "tp").astype(jnp.float32).sum(axis=0)
    out_tokens = (middle_copies[0].astype(jnp.float32) + down_out).astype(jnp.bfloat16).T
    return (out_tokens, new_c, new_n, new_m)


def solution(mesh):
    placed = (
        P("grp", ("kv", "tp")),
        P("kv"),
        P("kv", "tp"),
        P("kv", "tp"),
        P("kv", "tp"),
        P("kv", "tp"),
        P("kv", "tp"),
        P("kv", "tp"),
        P("tp"),
        P("tp"),
        P(("grp", "kv"), "tp", None, None),
        P(("grp", "kv"), "tp", None),
        P(("grp", "kv"), "tp"),
        P("tp", None),
        P("tp", "kv"),
        P("kv"),
        P("kv", "tp"),
        P("kv", "tp"),
        P("tp", "kv"),
    )
    return jax.shard_map(
        body,
        mesh=mesh,
        in_specs=placed,
        out_specs=(
            P("grp", ("kv", "tp")),
            P(("grp", "kv"), "tp", None, None),
            P(("grp", "kv"), "tp", None),
            P(("grp", "kv"), "tp"),
        ),
        check_vma=False,
    )
```

```python
import jax
import jax.numpy as jnp
from jax import lax
from jax.experimental import pallas as pl
from jax.experimental.pallas import tpu as pltpu
from jax.sharding import PartitionSpec as P

D = 4096
DK = 64
DV = 128
LANES = 128


norm_eps = 1e-06
igate_cap = 1.5

VMEM = pl.BlockSpec(memory_space=pltpu.VMEM)
ANY = pl.BlockSpec(memory_space=pl.ANY)
SMALL = pltpu.CompilerParams(vmem_limit_bytes=8 * 2**20)


def exchanged(blocks, axis):
    return lax.all_to_all(blocks, axis, split_axis=0, concat_axis=0, tiled=True)


def spread_kernel(value_ref, out_ref, own_ref):
    value = value_ref[...]
    own_ref[...] = value
    for copy in range(out_ref.shape[0]):
        out_ref[copy] = value


def spread(value, count):
    return pl.pallas_call(
        spread_kernel,
        out_shape=(
            jax.ShapeDtypeStruct((count, *value.shape), value.dtype),
            jax.ShapeDtypeStruct(value.shape, value.dtype),
        ),
        in_specs=[VMEM],
        out_specs=(VMEM, VMEM),
        compiler_params=SMALL,
        name="spread",
    )(value)


def transposed_product(x, weight):
    return lax.dot_general(
        x, weight, (((1,), (1,)), ((), ())), preferred_element_type=jnp.float32
    )


def project_kernel(
    x_ref, vectors_ref, small_ref, both_ref, value_ref, ogate_ref, out_ref, handed_ref
):
    handed_ref[...] = small_ref[...]
    x = x_ref[...].astype(jnp.float32).T
    normed = (x * vectors_ref[0:1, :]).astype(jnp.bfloat16)
    out_ref[:, :LANES] = transposed_product(normed, both_ref[...]).astype(out_ref.dtype)
    out_ref[:, LANES : 2 * LANES] = jnp.dot(
        normed, value_ref[...], preferred_element_type=jnp.float32
    ).astype(out_ref.dtype)
    out_ref[:, 2 * LANES : 3 * LANES] = jnp.dot(
        normed, ogate_ref[...], preferred_element_type=jnp.float32
    ).astype(out_ref.dtype)
    wide = normed.astype(jnp.float32)
    squares = jnp.sum(x * x, axis=1, keepdims=True)
    igate = jnp.sum(wide * vectors_ref[1:2, :], axis=1, keepdims=True)
    fgate = jnp.sum(wide * vectors_ref[2:3, :], axis=1, keepdims=True)
    lane = lax.broadcasted_iota(jnp.int32, (x.shape[0], LANES), 1)
    tail = jnp.where(
        lane == 0, igate, jnp.where(lane == 1, fgate, jnp.where(lane == 2, squares, 0.0))
    )
    out_ref[:, 3 * LANES :] = tail.astype(out_ref.dtype)


def project(x, vectors, small, w_both, w_value, w_ogate):
    return pl.pallas_call(
        project_kernel,
        out_shape=(
            jax.ShapeDtypeStruct((x.shape[1], 4 * LANES), jnp.bfloat16),
            jax.ShapeDtypeStruct(small.shape, small.dtype),
        ),
        in_specs=[VMEM] * 6,
        out_specs=(VMEM, VMEM),
        compiler_params=SMALL,
        name="project",
    )(x, vectors, small, w_both, w_value, w_ogate)


def cell_kernel(
    parts_ref, c_ref, small_ref,
    new_c_out, new_n_ref, new_m_ref, out_ref, new_c_ref, sems,
):
    total = parts_ref[0].astype(jnp.float32)
    for k in range(1, parts_ref.shape[0]):
        total += parts_ref[k].astype(jnp.float32)
    seqs = total.shape[0]
    tail = total[:, 3 * LANES :]
    row_scale = lax.rsqrt(tail[:, 2:3] / D + norm_eps)
    igate = igate_cap * jnp.tanh((row_scale * tail[:, 0:1] + small_ref[seqs + 2 : seqs + 3, 0:1]) / igate_cap)
    fgate = row_scale * tail[:, 1:2] + small_ref[seqs + 2 : seqs + 3, 1:2]
    diagonal = lax.broadcasted_iota(jnp.int32, (seqs, seqs), 0) == lax.broadcasted_iota(
        jnp.int32, (seqs, seqs), 1
    )
    state_m = jnp.sum(jnp.where(diagonal, small_ref[seqs : seqs + 1, :seqs], 0.0), axis=1, keepdims=True)
    log_keep = jnp.minimum(fgate, 0.0) - jnp.log1p(jnp.exp(-jnp.abs(fgate)))
    carried = log_keep + state_m
    new_m = jnp.maximum(carried, igate)
    keep = jnp.exp(carried - new_m)
    write = jnp.exp(igate - new_m)
    new_m_ref[...] = jnp.sum(jnp.where(diagonal, new_m, 0.0), axis=0, keepdims=True)
    lane = lax.broadcasted_iota(jnp.int32, (seqs, LANES), 1)
    first = total[:, :LANES]
    query_key = row_scale * jnp.where(lane < DK, first, first * DK ** (-0.5))
    query = query_key[:, :DK]
    key_vec = query_key[:, DK:]
    value_vec = row_scale * total[:, LANES : 2 * LANES]
    ogate = row_scale * total[:, 2 * LANES : 3 * LANES]
    new_n = keep * small_ref[:seqs, :DK] + write * key_vec
    new_n_ref[...] = new_n
    denominator = jnp.maximum(
        jnp.abs(jnp.sum(query * new_n, axis=1, keepdims=True)), jnp.exp(-new_m)
    )
    columns = jnp.where(lane < DK, query_key, write * query_key).T
    copies = []
    for b in range(seqs):
        key_b = columns[DK:, b : b + 1]
        new_c_ref[b] = keep[b : b + 1, :] * c_ref[b] + key_b * value_vec[b : b + 1, :]
        copies.append(pltpu.make_async_copy(new_c_ref.at[b], new_c_out.at[b], sems.at[b]))
        copies[b].start()
    rows = []
    for b in range(seqs):
        query_b = columns[:DK, b : b + 1]
        rows.append(jnp.sum(query_b * new_c_ref[b], axis=0, keepdims=True))
    head_out = jnp.concatenate(rows, axis=0) / denominator
    merged = head_out * small_ref[seqs + 1 : seqs + 2, :] / (1.0 + jnp.exp(-ogate))
    merged = merged.astype(out_ref.dtype)
    for copy in range(out_ref.shape[0]):
        out_ref[copy] = merged
    for copy in copies:
        copy.wait()


def cell(parts, state_c, small):
    count, seqs, _ = parts.shape
    new_c, new_n, new_m, out = pl.pallas_call(
        cell_kernel,
        out_shape=(
            jax.ShapeDtypeStruct((seqs, DK, DV), jnp.float32),
            jax.ShapeDtypeStruct((seqs, DK), jnp.float32),
            jax.ShapeDtypeStruct((1, seqs), jnp.float32),
            jax.ShapeDtypeStruct((count, seqs, DV), jnp.bfloat16),
        ),
        in_specs=[VMEM] * 3,
        out_specs=(ANY, VMEM, VMEM, VMEM),
        scratch_shapes=[
            pltpu.VMEM((seqs, DK, DV), jnp.float32),
            pltpu.SemaphoreType.DMA((seqs,)),
        ],
        compiler_params=SMALL,
        name="cell",
    )(
        parts, state_c.reshape(seqs, DK, DV), small,
    )
    return new_c.reshape(state_c.shape), new_n.reshape(seqs, 1, DK), new_m.T, out


def residual_kernel(parts_ref, tokens_ref, out_ref):
    total = parts_ref[0].astype(jnp.float32)
    for k in range(1, parts_ref.shape[0]):
        total += parts_ref[k].astype(jnp.float32)
    middle = (tokens_ref[...].astype(jnp.float32) + total).astype(out_ref.dtype)
    for copy in range(out_ref.shape[0]):
        out_ref[copy] = middle


def residual(parts, tokens):
    return pl.pallas_call(
        residual_kernel,
        out_shape=jax.ShapeDtypeStruct(parts.shape, parts.dtype),
        in_specs=[VMEM, VMEM],
        out_specs=VMEM,
        compiler_params=SMALL,
        name="residual",
    )(parts, tokens)


def widen_kernel(x_ref, vectors_ref, gate_ref, up_ref, out_ref):
    units = gate_ref.shape[0]
    cols = out_ref.shape[1]
    start = units // LANES * LANES
    taken = (LANES - (units - start)) % LANES
    x = x_ref[...].astype(jnp.float32).T
    normed = (x * vectors_ref[3:4, :]).astype(jnp.bfloat16)
    out_ref[:, :start] = transposed_product(normed, gate_ref[:start, :]).astype(out_ref.dtype)
    if taken:
        mixed = jnp.concatenate([gate_ref[start:, :], up_ref[:taken, :]], axis=0)
        out_ref[:, start : start + LANES] = transposed_product(normed, mixed).astype(
            out_ref.dtype
        )
        start += LANES
    filler = jnp.zeros((cols - 2 * units, gate_ref.shape[1]), gate_ref.dtype)
    rest = transposed_product(normed, jnp.concatenate([up_ref[taken:, :], filler], axis=0))
    lane = lax.broadcasted_iota(jnp.int32, rest.shape, 1)
    squares = jnp.sum(x * x, axis=1, keepdims=True)
    out_ref[:, start:] = jnp.where(lane == 2 * units - start, squares, rest).astype(out_ref.dtype)


def widen(x, vectors, w_gate, w_up):
    cols = (2 * w_gate.shape[1] // LANES + 1) * LANES
    return pl.pallas_call(
        widen_kernel,
        out_shape=jax.ShapeDtypeStruct((x.shape[1], cols), jnp.bfloat16),
        in_specs=[VMEM] * 4,
        out_specs=VMEM,
        compiler_params=SMALL,
        name="widen",
    )(x, vectors, w_gate.T, w_up.T)


def body(
    tokens,
    norm_gain,
    w_query,
    w_key,
    w_value,
    w_ogate,
    w_igate,
    w_fgate,
    igate_bias,
    fgate_bias,
    state_c,
    state_n,
    state_m,
    head_gain,
    w_out,
    ffn_gain,
    w_gate,
    w_up,
    w_down,
):
    n_kv, n_tp = lax.axis_size("kv"), lax.axis_size("tp")
    seqs, feats = tokens.shape
    units = w_gate.shape[1]
    rows = n_tp * feats
    own_seqs = seqs // n_kv

    wide = [norm_gain[None], w_igate.T, w_fgate.T, ffn_gain[None]]
    vectors = jnp.concatenate(wide, axis=0).astype(jnp.float32)
    narrow = [
        state_n.reshape(own_seqs, DK), state_m.T, head_gain.astype(jnp.float32),
        jnp.stack([igate_bias, fgate_bias], axis=1),
    ]
    small = jnp.concatenate(
        [jnp.pad(one, ((0, 0), (0, LANES - one.shape[1]))) for one in narrow], axis=0
    )
    token_copies, own_tokens = spread(tokens.T, n_tp)
    token_rows = exchanged(token_copies, "tp").reshape(rows, seqs)
    w_both = jnp.concatenate([w_query.T, w_key.T], axis=0)
    parts, small = project(token_rows, vectors, small, w_both, w_value, w_ogate)
    arrived = exchanged(parts.reshape(n_kv, own_seqs, -1), "kv")
    new_c, new_n, new_m, merged = cell(arrived, state_c, small)
    merged_all = exchanged(merged, "kv").reshape(seqs, -1)
    attn_part = jnp.dot(merged_all, w_out, preferred_element_type=jnp.float32)
    attn_part = attn_part.astype(jnp.bfloat16).T.reshape(n_tp, feats, seqs)
    middle_copies = residual(exchanged(attn_part, "tp"), own_tokens)
    middle_rows = exchanged(middle_copies, "tp").reshape(rows, seqs)
    spread_out = widen(middle_rows, vectors, w_gate, w_up)
    sums = exchanged(spread_out.reshape(n_kv, own_seqs, -1), "kv").astype(jnp.float32).sum(axis=0)
    gate_sum, up_sum, total = sums[:, :units], sums[:, units : 2 * units], sums[:, 2 * units]
    ffn_scale = lax.rsqrt(total / D + norm_eps)[:, None]
    hidden = (jax.nn.silu(ffn_scale * gate_sum) * (ffn_scale * up_sum)).astype(jnp.bfloat16)
    hidden_all = exchanged(
        jnp.broadcast_to(hidden[None], (n_kv, *hidden.shape)), "kv"
    ).reshape(seqs, units)
    down_part = jnp.dot(hidden_all, w_down, preferred_element_type=jnp.float32)
    down_part = down_part.astype(jnp.bfloat16).T.reshape(n_tp, feats, seqs)
    down_out = exchanged(down_part, "tp").astype(jnp.float32).sum(axis=0)
    out_tokens = (middle_copies[0].astype(jnp.float32) + down_out).astype(jnp.bfloat16).T
    return (out_tokens, new_c, new_n, new_m)


def solution(mesh):
    placed = (
        P("grp", ("kv", "tp")),
        P("kv"),
        P("kv", "tp"),
        P("kv", "tp"),
        P("kv", "tp"),
        P("kv", "tp"),
        P("kv", "tp"),
        P("kv", "tp"),
        P("tp"),
        P("tp"),
        P(("grp", "kv"), "tp", None, None),
        P(("grp", "kv"), "tp", None),
        P(("grp", "kv"), "tp"),
        P("tp", None),
        P("tp", "kv"),
        P("kv"),
        P("kv", "tp"),
        P("kv", "tp"),
        P("tp", "kv"),
    )
    return jax.shard_map(
        body,
        mesh=mesh,
        in_specs=placed,
        out_specs=(
            P("grp", ("kv", "tp")),
            P(("grp", "kv"), "tp", None, None),
            P(("grp", "kv"), "tp", None),
            P(("grp", "kv"), "tp"),
        ),
        check_vma=False,
    )
```

```python
import jax
import jax.numpy as jnp
from jax import lax
from jax.experimental import pallas as pl
from jax.experimental.pallas import tpu as pltpu
from jax.sharding import PartitionSpec as P

D = 4096
DK = 64
DV = 128
LANES = 128


norm_eps = 1e-06
igate_cap = 1.5

VMEM = pl.BlockSpec(memory_space=pltpu.VMEM)
ANY = pl.BlockSpec(memory_space=pl.ANY)
SMALL = pltpu.CompilerParams(vmem_limit_bytes=8 * 2**20)


def exchanged(blocks, axis):
    return lax.all_to_all(blocks, axis, split_axis=0, concat_axis=0, tiled=True)


def spread_kernel(value_ref, out_ref, own_ref):
    value = value_ref[...]
    own_ref[...] = value
    for copy in range(out_ref.shape[0]):
        out_ref[copy] = value


def spread(value, count):
    return pl.pallas_call(
        spread_kernel,
        out_shape=(
            jax.ShapeDtypeStruct((count, *value.shape), value.dtype),
            jax.ShapeDtypeStruct(value.shape, value.dtype),
        ),
        in_specs=[VMEM],
        out_specs=(VMEM, VMEM),
        compiler_params=SMALL,
        name="spread",
    )(value)


def transposed_product(x, weight):
    return lax.dot_general(
        x, weight, (((1,), (1,)), ((), ())), preferred_element_type=jnp.float32
    )


def project_kernel(
    x_ref, vectors_ref, small_ref, both_ref, value_ref, ogate_ref, out_ref, handed_ref
):
    handed_ref[...] = small_ref[...]
    x = x_ref[...].astype(jnp.float32).T
    normed = (x * vectors_ref[0:1, :]).astype(jnp.bfloat16)
    out_ref[:, :LANES] = transposed_product(normed, both_ref[...]).astype(out_ref.dtype)
    out_ref[:, LANES : 2 * LANES] = jnp.dot(
        normed, value_ref[...], preferred_element_type=jnp.float32
    ).astype(out_ref.dtype)
    out_ref[:, 2 * LANES : 3 * LANES] = jnp.dot(
        normed, ogate_ref[...], preferred_element_type=jnp.float32
    ).astype(out_ref.dtype)
    wide = normed.astype(jnp.float32)
    squares = jnp.sum(x * x, axis=1, keepdims=True)
    igate = jnp.sum(wide * vectors_ref[1:2, :], axis=1, keepdims=True)
    fgate = jnp.sum(wide * vectors_ref[2:3, :], axis=1, keepdims=True)
    lane = lax.broadcasted_iota(jnp.int32, (x.shape[0], LANES), 1)
    tail = jnp.where(
        lane == 0, igate, jnp.where(lane == 1, fgate, jnp.where(lane == 2, squares, 0.0))
    )
    out_ref[:, 3 * LANES :] = tail.astype(out_ref.dtype)


def project(x, vectors, small, w_both, w_value, w_ogate):
    return pl.pallas_call(
        project_kernel,
        out_shape=(
            jax.ShapeDtypeStruct((x.shape[1], 4 * LANES), jnp.bfloat16),
            jax.ShapeDtypeStruct(small.shape, small.dtype),
        ),
        in_specs=[VMEM] * 6,
        out_specs=(VMEM, VMEM),
        compiler_params=SMALL,
        name="project",
    )(x, vectors, small, w_both, w_value, w_ogate)


def cell_kernel(
    parts_ref, c_ref, small_ref,
    new_c_ref, new_n_ref, new_m_ref, out_ref,
):
    total = parts_ref[0].astype(jnp.float32)
    for k in range(1, parts_ref.shape[0]):
        total += parts_ref[k].astype(jnp.float32)
    seqs = total.shape[0]
    tail = total[:, 3 * LANES :]
    row_scale = lax.rsqrt(tail[:, 2:3] / D + norm_eps)
    igate = igate_cap * jnp.tanh((row_scale * tail[:, 0:1] + small_ref[seqs + 2 : seqs + 3, 0:1]) / igate_cap)
    fgate = row_scale * tail[:, 1:2] + small_ref[seqs + 2 : seqs + 3, 1:2]
    diagonal = lax.broadcasted_iota(jnp.int32, (seqs, seqs), 0) == lax.broadcasted_iota(
        jnp.int32, (seqs, seqs), 1
    )
    state_m = jnp.sum(jnp.where(diagonal, small_ref[seqs : seqs + 1, :seqs], 0.0), axis=1, keepdims=True)
    log_keep = jnp.minimum(fgate, 0.0) - jnp.log1p(jnp.exp(-jnp.abs(fgate)))
    carried = log_keep + state_m
    new_m = jnp.maximum(carried, igate)
    keep = jnp.exp(carried - new_m)
    write = jnp.exp(igate - new_m)
    new_m_ref[...] = jnp.sum(jnp.where(diagonal, new_m, 0.0), axis=0, keepdims=True)
    lane = lax.broadcasted_iota(jnp.int32, (seqs, LANES), 1)
    first = total[:, :LANES]
    query_key = row_scale * jnp.where(lane < DK, first, first * DK ** (-0.5))
    query = query_key[:, :DK]
    key_vec = query_key[:, DK:]
    value_vec = row_scale * total[:, LANES : 2 * LANES]
    ogate = row_scale * total[:, 2 * LANES : 3 * LANES]
    new_n = keep * small_ref[:seqs, :DK] + write * key_vec
    new_n_ref[...] = new_n
    denominator = jnp.maximum(
        jnp.abs(jnp.sum(query * new_n, axis=1, keepdims=True)), jnp.exp(-new_m)
    )
    columns = jnp.where(lane < DK, query_key, write * query_key).T
    rows = []
    for b in range(seqs):
        query_b = columns[:DK, b : b + 1]
        key_b = columns[DK:, b : b + 1]
        new_c = keep[b : b + 1, :] * c_ref[b] + key_b * value_vec[b : b + 1, :]
        new_c_ref[b] = new_c
        rows.append(jnp.sum(query_b * new_c, axis=0, keepdims=True))
    head_out = jnp.concatenate(rows, axis=0) / denominator
    merged = head_out * small_ref[seqs + 1 : seqs + 2, :] / (1.0 + jnp.exp(-ogate))
    merged = merged.astype(out_ref.dtype)
    for copy in range(out_ref.shape[0]):
        out_ref[copy] = merged


def cell(parts, state_c, small):
    count, seqs, _ = parts.shape
    new_c, new_n, new_m, out = pl.pallas_call(
        cell_kernel,
        out_shape=(
            jax.ShapeDtypeStruct((seqs, DK, DV), jnp.float32),
            jax.ShapeDtypeStruct((seqs, DK), jnp.float32),
            jax.ShapeDtypeStruct((1, seqs), jnp.float32),
            jax.ShapeDtypeStruct((count, seqs, DV), jnp.bfloat16),
        ),
        in_specs=[VMEM] * 3,
        out_specs=(VMEM,) * 4,
        compiler_params=SMALL,
        name="cell",
    )(
        parts, state_c.reshape(seqs, DK, DV), small,
    )
    return (new_c, new_n, new_m), out


def residual_kernel(parts_ref, tokens_ref, out_ref):
    total = parts_ref[0].astype(jnp.float32)
    for k in range(1, parts_ref.shape[0]):
        total += parts_ref[k].astype(jnp.float32)
    middle = (tokens_ref[...].astype(jnp.float32) + total).astype(out_ref.dtype)
    for copy in range(out_ref.shape[0]):
        out_ref[copy] = middle


def residual(parts, tokens):
    return pl.pallas_call(
        residual_kernel,
        out_shape=jax.ShapeDtypeStruct(parts.shape, parts.dtype),
        in_specs=[VMEM, VMEM],
        out_specs=VMEM,
        compiler_params=SMALL,
        name="residual",
    )(parts, tokens)


def finish_kernel(parts_ref, middle_ref, *refs):
    count = (len(refs) - 3) // 2
    states, out_ref, targets = refs[:count], refs[count], refs[count + 1 : -2]
    tokens, sems = refs[-2:]
    copies = [
        pltpu.make_async_copy(state, target, sems.at[k])
        for k, (state, target) in enumerate(zip(states, targets))
    ]
    for copy in copies:
        copy.start()
    total = parts_ref[0].astype(jnp.float32)
    for k in range(1, parts_ref.shape[0]):
        total += parts_ref[k].astype(jnp.float32)
    tokens[...] = (middle_ref[0].astype(jnp.float32) + total).astype(tokens.dtype)
    copies.append(pltpu.make_async_copy(tokens, out_ref, sems.at[count]))
    copies[count].start()
    for copy in copies:
        copy.wait()


def finish(parts, middle, *states):
    return pl.pallas_call(
        finish_kernel,
        out_shape=(
            jax.ShapeDtypeStruct(parts.shape[1:], parts.dtype),
            *(jax.ShapeDtypeStruct(one.shape, one.dtype) for one in states),
        ),
        in_specs=[VMEM] * (2 + len(states)),
        out_specs=(ANY,) * (1 + len(states)),
        scratch_shapes=[
            pltpu.VMEM(parts.shape[1:], parts.dtype),
            pltpu.SemaphoreType.DMA((1 + len(states),)),
        ],
        compiler_params=SMALL,
        name="finish",
    )(parts, middle, *states)


def widen_kernel(x_ref, vectors_ref, gate_ref, up_ref, out_ref):
    units = gate_ref.shape[0]
    cols = out_ref.shape[1]
    start = units // LANES * LANES
    taken = (LANES - (units - start)) % LANES
    x = x_ref[...].astype(jnp.float32).T
    normed = (x * vectors_ref[3:4, :]).astype(jnp.bfloat16)
    out_ref[:, :start] = transposed_product(normed, gate_ref[:start, :]).astype(out_ref.dtype)
    if taken:
        mixed = jnp.concatenate([gate_ref[start:, :], up_ref[:taken, :]], axis=0)
        out_ref[:, start : start + LANES] = transposed_product(normed, mixed).astype(
            out_ref.dtype
        )
        start += LANES
    filler = jnp.zeros((cols - 2 * units, gate_ref.shape[1]), gate_ref.dtype)
    rest = transposed_product(normed, jnp.concatenate([up_ref[taken:, :], filler], axis=0))
    lane = lax.broadcasted_iota(jnp.int32, rest.shape, 1)
    squares = jnp.sum(x * x, axis=1, keepdims=True)
    out_ref[:, start:] = jnp.where(lane == 2 * units - start, squares, rest).astype(out_ref.dtype)


def widen(x, vectors, w_gate, w_up):
    cols = (2 * w_gate.shape[1] // LANES + 1) * LANES
    return pl.pallas_call(
        widen_kernel,
        out_shape=jax.ShapeDtypeStruct((x.shape[1], cols), jnp.bfloat16),
        in_specs=[VMEM] * 4,
        out_specs=VMEM,
        compiler_params=SMALL,
        name="widen",
    )(x, vectors, w_gate.T, w_up.T)


def body(
    tokens,
    norm_gain,
    w_query,
    w_key,
    w_value,
    w_ogate,
    w_igate,
    w_fgate,
    igate_bias,
    fgate_bias,
    state_c,
    state_n,
    state_m,
    head_gain,
    w_out,
    ffn_gain,
    w_gate,
    w_up,
    w_down,
):
    n_kv, n_tp = lax.axis_size("kv"), lax.axis_size("tp")
    seqs, feats = tokens.shape
    units = w_gate.shape[1]
    rows = n_tp * feats
    own_seqs = seqs // n_kv

    wide = [norm_gain[None], w_igate.T, w_fgate.T, ffn_gain[None]]
    vectors = jnp.concatenate(wide, axis=0).astype(jnp.float32)
    narrow = [
        state_n.reshape(own_seqs, DK), state_m.T, head_gain.astype(jnp.float32),
        jnp.stack([igate_bias, fgate_bias], axis=1),
    ]
    small = jnp.concatenate(
        [jnp.pad(one, ((0, 0), (0, LANES - one.shape[1]))) for one in narrow], axis=0
    )
    token_copies, own_tokens = spread(tokens.T, n_tp)
    token_rows = exchanged(token_copies, "tp").reshape(rows, seqs)
    w_both = jnp.concatenate([w_query.T, w_key.T], axis=0)
    parts, small = project(token_rows, vectors, small, w_both, w_value, w_ogate)
    arrived = exchanged(parts.reshape(n_kv, own_seqs, -1), "kv")
    states, merged = cell(arrived, state_c, small)
    merged_all = exchanged(merged, "kv").reshape(seqs, -1)
    attn_part = jnp.dot(merged_all, w_out, preferred_element_type=jnp.float32)
    attn_part = attn_part.astype(jnp.bfloat16).T.reshape(n_tp, feats, seqs)
    middle_copies = residual(exchanged(attn_part, "tp"), own_tokens)
    middle_rows = exchanged(middle_copies, "tp").reshape(rows, seqs)
    spread_out = widen(middle_rows, vectors, w_gate, w_up)
    sums = exchanged(spread_out.reshape(n_kv, own_seqs, -1), "kv").astype(jnp.float32).sum(axis=0)
    gate_sum, up_sum, total = sums[:, :units], sums[:, units : 2 * units], sums[:, 2 * units]
    ffn_scale = lax.rsqrt(total / D + norm_eps)[:, None]
    hidden = (jax.nn.silu(ffn_scale * gate_sum) * (ffn_scale * up_sum)).astype(jnp.bfloat16)
    hidden_all = exchanged(
        jnp.broadcast_to(hidden[None], (n_kv, *hidden.shape)), "kv"
    ).reshape(seqs, units)
    down_part = jnp.dot(hidden_all, w_down, preferred_element_type=jnp.float32)
    down_part = down_part.astype(jnp.bfloat16).T.reshape(n_tp, feats, seqs)
    out_tokens, new_c, new_n, new_m = finish(
        exchanged(down_part, "tp"), middle_copies, *states
    )
    new_n = new_n.reshape(own_seqs, 1, DK)
    return (out_tokens.T, new_c.reshape(state_c.shape), new_n, new_m.T)


def solution(mesh):
    placed = (
        P("grp", ("kv", "tp")),
        P("kv"),
        P("kv", "tp"),
        P("kv", "tp"),
        P("kv", "tp"),
        P("kv", "tp"),
        P("kv", "tp"),
        P("kv", "tp"),
        P("tp"),
        P("tp"),
        P(("grp", "kv"), "tp", None, None),
        P(("grp", "kv"), "tp", None),
        P(("grp", "kv"), "tp"),
        P("tp", None),
        P("tp", "kv"),
        P("kv"),
        P("kv", "tp"),
        P("kv", "tp"),
        P("tp", "kv"),
    )
    return jax.shard_map(
        body,
        mesh=mesh,
        in_specs=placed,
        out_specs=(
            P("grp", ("kv", "tp")),
            P(("grp", "kv"), "tp", None, None),
            P(("grp", "kv"), "tp", None),
            P(("grp", "kv"), "tp"),
        ),
        check_vma=False,
    )
```

```python
import functools

import jax
import jax.numpy as jnp
from jax import lax
from jax.experimental import pallas as pl
from jax.experimental.pallas import tpu as pltpu
from jax.sharding import PartitionSpec as P

D = 4096
DK = 64
DV = 128
LANES = 128


norm_eps = 1e-06
igate_cap = 1.5

VMEM = pl.BlockSpec(memory_space=pltpu.VMEM)
ANY = pl.BlockSpec(memory_space=pl.ANY)
SMALL = pltpu.CompilerParams(vmem_limit_bytes=8 * 2**20)


def exchanged(blocks, axis, groups=None):
    return lax.all_to_all(
        blocks, axis, split_axis=0, concat_axis=0, tiled=True, axis_index_groups=groups
    )


def spread_kernel(value_ref, out_ref, own_ref):
    value = value_ref[...]
    own_ref[...] = value
    for copy in range(out_ref.shape[0]):
        out_ref[copy] = value


def spread(value, count):
    return pl.pallas_call(
        spread_kernel,
        out_shape=(
            jax.ShapeDtypeStruct((count, *value.shape), value.dtype),
            jax.ShapeDtypeStruct(value.shape, value.dtype),
        ),
        in_specs=[VMEM],
        out_specs=(VMEM, VMEM),
        compiler_params=SMALL,
        name="spread",
    )(value)


def transposed_product(x, weight):
    return lax.dot_general(
        x, weight, (((1,), (1,)), ((), ())), preferred_element_type=jnp.float32
    )


def project_kernel(
    x_ref, vectors_ref, small_ref, both_ref, value_ref, ogate_ref, out_ref, handed_ref
):
    handed_ref[...] = small_ref[...]
    x = x_ref[...].astype(jnp.float32).T
    normed = (x * vectors_ref[0:1, :]).astype(jnp.bfloat16)
    out_ref[:, :LANES] = transposed_product(normed, both_ref[...]).astype(out_ref.dtype)
    out_ref[:, LANES : 2 * LANES] = jnp.dot(
        normed, value_ref[...], preferred_element_type=jnp.float32
    ).astype(out_ref.dtype)
    out_ref[:, 2 * LANES : 3 * LANES] = jnp.dot(
        normed, ogate_ref[...], preferred_element_type=jnp.float32
    ).astype(out_ref.dtype)
    wide = normed.astype(jnp.float32)
    squares = jnp.sum(x * x, axis=1, keepdims=True)
    igate = jnp.sum(wide * vectors_ref[1:2, :], axis=1, keepdims=True)
    fgate = jnp.sum(wide * vectors_ref[2:3, :], axis=1, keepdims=True)
    lane = lax.broadcasted_iota(jnp.int32, (x.shape[0], LANES), 1)
    tail = jnp.where(
        lane == 0, igate, jnp.where(lane == 1, fgate, jnp.where(lane == 2, squares, 0.0))
    )
    out_ref[:, 3 * LANES :] = tail.astype(out_ref.dtype)


def project(x, vectors, small, w_both, w_value, w_ogate):
    return pl.pallas_call(
        project_kernel,
        out_shape=(
            jax.ShapeDtypeStruct((x.shape[1], 4 * LANES), jnp.bfloat16),
            jax.ShapeDtypeStruct(small.shape, small.dtype),
        ),
        in_specs=[VMEM] * 6,
        out_specs=(VMEM, VMEM),
        compiler_params=SMALL,
        name="project",
    )(x, vectors, small, w_both, w_value, w_ogate)


def cell_kernel(
    parts_ref, c_ref, small_ref,
    new_c_ref, new_n_ref, new_m_ref, out_ref,
):
    total = parts_ref[0].astype(jnp.float32)
    for k in range(1, parts_ref.shape[0]):
        total += parts_ref[k].astype(jnp.float32)
    seqs = total.shape[0]
    tail = total[:, 3 * LANES :]
    row_scale = lax.rsqrt(tail[:, 2:3] / D + norm_eps)
    igate = igate_cap * jnp.tanh((row_scale * tail[:, 0:1] + small_ref[seqs + 2 : seqs + 3, 0:1]) / igate_cap)
    fgate = row_scale * tail[:, 1:2] + small_ref[seqs + 2 : seqs + 3, 1:2]
    diagonal = lax.broadcasted_iota(jnp.int32, (seqs, seqs), 0) == lax.broadcasted_iota(
        jnp.int32, (seqs, seqs), 1
    )
    state_m = jnp.sum(jnp.where(diagonal, small_ref[seqs : seqs + 1, :seqs], 0.0), axis=1, keepdims=True)
    log_keep = jnp.minimum(fgate, 0.0) - jnp.log1p(jnp.exp(-jnp.abs(fgate)))
    carried = log_keep + state_m
    new_m = jnp.maximum(carried, igate)
    keep = jnp.exp(carried - new_m)
    write = jnp.exp(igate - new_m)
    new_m_ref[...] = jnp.sum(jnp.where(diagonal, new_m, 0.0), axis=0, keepdims=True)
    lane = lax.broadcasted_iota(jnp.int32, (seqs, LANES), 1)
    first = total[:, :LANES]
    query_key = row_scale * jnp.where(lane < DK, first, first * DK ** (-0.5))
    query = query_key[:, :DK]
    key_vec = query_key[:, DK:]
    value_vec = row_scale * total[:, LANES : 2 * LANES]
    ogate = row_scale * total[:, 2 * LANES : 3 * LANES]
    new_n = keep * small_ref[:seqs, :DK] + write * key_vec
    new_n_ref[...] = new_n
    denominator = jnp.maximum(
        jnp.abs(jnp.sum(query * new_n, axis=1, keepdims=True)), jnp.exp(-new_m)
    )
    columns = jnp.where(lane < DK, query_key, write * query_key).T
    rows = []
    for b in range(seqs):
        query_b = columns[:DK, b : b + 1]
        key_b = columns[DK:, b : b + 1]
        new_c = keep[b : b + 1, :] * c_ref[b] + key_b * value_vec[b : b + 1, :]
        new_c_ref[b] = new_c
        rows.append(jnp.sum(query_b * new_c, axis=0, keepdims=True))
    head_out = jnp.concatenate(rows, axis=0) / denominator
    merged = head_out * small_ref[seqs + 1 : seqs + 2, :] / (1.0 + jnp.exp(-ogate))
    merged = merged.astype(out_ref.dtype)
    for copy in range(out_ref.shape[0]):
        out_ref[copy] = merged


def cell(parts, state_c, small):
    count, seqs, _ = parts.shape
    new_c, new_n, new_m, out = pl.pallas_call(
        cell_kernel,
        out_shape=(
            jax.ShapeDtypeStruct((seqs, DK, DV), jnp.float32),
            jax.ShapeDtypeStruct((seqs, DK), jnp.float32),
            jax.ShapeDtypeStruct((1, seqs), jnp.float32),
            jax.ShapeDtypeStruct((count, seqs, DV), jnp.bfloat16),
        ),
        in_specs=[VMEM] * 3,
        out_specs=(VMEM,) * 4,
        compiler_params=SMALL,
        name="cell",
    )(
        parts, state_c.reshape(seqs, DK, DV), small,
    )
    return (new_c, new_n, new_m), out


def residual_kernel(parts_ref, tokens_ref, own_ref, out_ref):
    total = parts_ref[0].astype(jnp.float32)
    for k in range(1, parts_ref.shape[0]):
        total += parts_ref[k].astype(jnp.float32)
    middle = (tokens_ref[...].astype(jnp.float32) + total).astype(own_ref.dtype)
    own_ref[...] = middle
    middle = middle.astype(jnp.float32)
    feats, seqs = middle.shape
    copies = out_ref.shape[0] // 2
    for half in range(2):
        at = half * (seqs // 2)
        picked = middle[:, at : at + seqs // 2]
        packed = jnp.concatenate([picked[: feats // 2], picked[feats // 2 :]], axis=1)
        packed = packed.astype(out_ref.dtype)
        for copy in range(copies):
            out_ref[half * copies + copy] = packed


def residual(parts, tokens):
    count, feats, seqs = parts.shape
    return pl.pallas_call(
        residual_kernel,
        out_shape=(
            jax.ShapeDtypeStruct((feats, seqs), parts.dtype),
            jax.ShapeDtypeStruct((2 * count, feats // 2, seqs), parts.dtype),
        ),
        in_specs=[VMEM, VMEM],
        out_specs=(VMEM, VMEM),
        compiler_params=SMALL,
        name="residual",
    )(parts, tokens)


def finish_kernel(parts_ref, middle_ref, *refs):
    count = (len(refs) - 3) // 2
    states, out_ref, targets = refs[:count], refs[count], refs[count + 1 : -2]
    tokens, sems = refs[-2:]
    copies = [
        pltpu.make_async_copy(state, target, sems.at[k])
        for k, (state, target) in enumerate(zip(states, targets))
    ]
    for copy in copies:
        copy.start()
    total = parts_ref[0].astype(jnp.float32)
    for k in range(1, parts_ref.shape[0]):
        total += parts_ref[k].astype(jnp.float32)
    tokens[...] = (middle_ref[...].astype(jnp.float32) + total).astype(tokens.dtype)
    copies.append(pltpu.make_async_copy(tokens, out_ref, sems.at[count]))
    copies[count].start()
    for copy in copies:
        copy.wait()


def finish(parts, middle, *states):
    return pl.pallas_call(
        finish_kernel,
        out_shape=(
            jax.ShapeDtypeStruct(parts.shape[1:], parts.dtype),
            *(jax.ShapeDtypeStruct(one.shape, one.dtype) for one in states),
        ),
        in_specs=[VMEM] * (2 + len(states)),
        out_specs=(ANY,) * (1 + len(states)),
        scratch_shapes=[
            pltpu.VMEM(parts.shape[1:], parts.dtype),
            pltpu.SemaphoreType.DMA((1 + len(states),)),
        ],
        compiler_params=SMALL,
        name="finish",
    )(parts, middle, *states)


def widen_kernel(units, x_ref, vectors_ref, own_ref, other_ref, out_ref):
    blocks = x_ref.shape[0] // 2
    half = x_ref.shape[2] // 2
    cols = out_ref.shape[1]
    place = lax.rem(lax.axis_index("kv"), 2)

    def features(which):
        packed = x_ref[pl.ds(which * blocks, blocks)].astype(jnp.float32)
        both = jnp.concatenate([packed[:, :, :half], packed[:, :, half:]], axis=1)
        return both.reshape(-1, half).T

    last = cols - LANES
    own, other = features(place), features(1 - place)
    squares = jnp.sum(own * own, axis=1, keepdims=True) + jnp.sum(
        other * other, axis=1, keepdims=True
    )
    own = (own * vectors_ref[3:4, :]).astype(jnp.bfloat16)
    gain = other_ref[units : units + 1, :].astype(jnp.float32)
    other = (other * gain).astype(jnp.bfloat16)
    out_ref[:, :last] = (
        transposed_product(own, own_ref[:last, :]) + transposed_product(other, other_ref[:last, :])
    ).astype(out_ref.dtype)
    rest = transposed_product(own, own_ref[last:, :]) + transposed_product(
        other, other_ref[last:, :]
    )
    lane = lax.broadcasted_iota(jnp.int32, rest.shape, 1)
    out_ref[:, last:] = jnp.where(lane == units - last, squares, rest).astype(out_ref.dtype)


def widen(x, vectors, own, other, units):
    return pl.pallas_call(
        functools.partial(widen_kernel, units),
        out_shape=jax.ShapeDtypeStruct((x.shape[2] // 2, own.shape[0]), jnp.bfloat16),
        in_specs=[VMEM] * 4,
        out_specs=VMEM,
        compiler_params=SMALL,
        name="widen",
    )(x, vectors, own, other)


def body(
    tokens,
    norm_gain,
    w_query,
    w_key,
    w_value,
    w_ogate,
    w_igate,
    w_fgate,
    igate_bias,
    fgate_bias,
    state_c,
    state_n,
    state_m,
    head_gain,
    w_out,
    ffn_gain,
    w_gate,
    w_up,
    w_down,
):
    n_kv, n_tp = lax.axis_size("kv"), lax.axis_size("tp")
    seqs, feats = tokens.shape
    units = w_gate.shape[1]
    rows = n_tp * feats
    own_seqs = seqs // n_kv

    wide = [norm_gain[None], w_igate.T, w_fgate.T, ffn_gain[None]]
    vectors = jnp.concatenate(wide, axis=0).astype(jnp.float32)
    narrow = [
        state_n.reshape(own_seqs, DK), state_m.T, head_gain.astype(jnp.float32),
        jnp.stack([igate_bias, fgate_bias], axis=1),
    ]
    small = jnp.concatenate(
        [jnp.pad(one, ((0, 0), (0, LANES - one.shape[1]))) for one in narrow], axis=0
    )
    shared = [w_gate.T, w_up.T, ffn_gain[None]]
    cols = (2 * units // LANES + 1) * LANES
    shared.append(jnp.zeros((cols - 2 * units - 1, rows), jnp.bfloat16))
    own_weights = jnp.concatenate(shared, axis=0)
    token_copies, own_tokens = spread(tokens.T, n_tp)
    token_rows = exchanged(token_copies, "tp").reshape(rows, seqs)
    token_rows, own_weights = lax.optimization_barrier((token_rows, own_weights))
    w_both = jnp.concatenate([w_query.T, w_key.T], axis=0)
    parts, small = project(token_rows, vectors, small, w_both, w_value, w_ogate)
    arrived = exchanged(parts.reshape(n_kv, own_seqs, -1), "kv")
    states, merged = cell(arrived, state_c, small)
    merged_all = exchanged(merged, "kv").reshape(seqs, -1)
    merged_all, own_weights = lax.optimization_barrier((merged_all, own_weights))
    swap = [(k, k + 1 - 2 * (k % 2)) for k in range(n_kv)]
    other_weights = lax.ppermute(own_weights, "kv", swap)
    attn_part = jnp.dot(merged_all, w_out, preferred_element_type=jnp.float32)
    attn_part = attn_part.astype(jnp.bfloat16).T.reshape(n_tp, feats, seqs)
    own_middle, middle_copies = residual(exchanged(attn_part, "tp"), own_tokens)
    pairs = [[k * n_tp + t for t in range(2 * n_tp)] for k in range(0, n_kv, 2)]
    middle_rows = exchanged(middle_copies, ("kv", "tp"), pairs)
    partial = widen(middle_rows, vectors, own_weights, other_weights, 2 * units)
    halves = [list(range(place, n_kv, 2)) for place in range(2)]
    arrived = exchanged(partial.reshape(n_kv // 2, own_seqs, -1), "kv", halves)
    sums = arrived.astype(jnp.float32).sum(axis=0)
    gate_sum, up_sum, total = sums[:, :units], sums[:, units : 2 * units], sums[:, 2 * units]
    ffn_scale = lax.rsqrt(total / D + norm_eps)[:, None]
    hidden = (jax.nn.silu(ffn_scale * gate_sum) * (ffn_scale * up_sum)).astype(jnp.bfloat16)
    hidden_all = exchanged(
        jnp.broadcast_to(hidden[None], (n_kv, *hidden.shape)), "kv", [halves[0] + halves[1]]
    ).reshape(seqs, units)
    down_part = jnp.dot(hidden_all, w_down, preferred_element_type=jnp.float32)
    down_part = down_part.astype(jnp.bfloat16).T.reshape(n_tp, feats, seqs)
    out_tokens, new_c, new_n, new_m = finish(
        exchanged(down_part, "tp"), own_middle, *states
    )
    new_n = new_n.reshape(own_seqs, 1, DK)
    return (out_tokens.T, new_c.reshape(state_c.shape), new_n, new_m.T)


def solution(mesh):
    placed = (
        P("grp", ("kv", "tp")),
        P("kv"),
        P("kv", "tp"),
        P("kv", "tp"),
        P("kv", "tp"),
        P("kv", "tp"),
        P("kv", "tp"),
        P("kv", "tp"),
        P("tp"),
        P("tp"),
        P(("grp", "kv"), "tp", None, None),
        P(("grp", "kv"), "tp", None),
        P(("grp", "kv"), "tp"),
        P("tp", None),
        P("tp", "kv"),
        P("kv"),
        P("kv", "tp"),
        P("kv", "tp"),
        P("tp", "kv"),
    )
    return jax.shard_map(
        body,
        mesh=mesh,
        in_specs=placed,
        out_specs=(
            P("grp", ("kv", "tp")),
            P(("grp", "kv"), "tp", None, None),
            P(("grp", "kv"), "tp", None),
            P(("grp", "kv"), "tp"),
        ),
        check_vma=False,
    )
```

```python
import functools

import jax
import jax.numpy as jnp
from jax import lax
from jax.experimental import pallas as pl
from jax.experimental.pallas import tpu as pltpu
from jax.sharding import PartitionSpec as P

D = 4096
DK = 64
DV = 128
LANES = 128


norm_eps = 1e-06
igate_cap = 1.5

VMEM = pl.BlockSpec(memory_space=pltpu.VMEM)
ANY = pl.BlockSpec(memory_space=pl.ANY)
SMALL = pltpu.CompilerParams(vmem_limit_bytes=8 * 2**20)


def exchanged(blocks, axis, groups=None):
    return lax.all_to_all(
        blocks, axis, split_axis=0, concat_axis=0, tiled=True, axis_index_groups=groups
    )


def spread_kernel(value_ref, out_ref, own_ref):
    value = value_ref[...]
    own_ref[...] = value
    for copy in range(out_ref.shape[0]):
        out_ref[copy] = value


def spread(value, count):
    return pl.pallas_call(
        spread_kernel,
        out_shape=(
            jax.ShapeDtypeStruct((count, *value.shape), value.dtype),
            jax.ShapeDtypeStruct(value.shape, value.dtype),
        ),
        in_specs=[VMEM],
        out_specs=(VMEM, VMEM),
        compiler_params=SMALL,
        name="spread",
    )(value)


def transposed_product(x, weight):
    return lax.dot_general(
        x, weight, (((1,), (1,)), ((), ())), preferred_element_type=jnp.float32
    )


def project_kernel(
    x_ref, vectors_ref, small_ref, both_ref, value_ref, ogate_ref, out_ref, handed_ref
):
    handed_ref[...] = small_ref[...]
    x = x_ref[...].astype(jnp.float32).T
    normed = (x * vectors_ref[0:1, :]).astype(jnp.bfloat16)
    out_ref[:, :LANES] = transposed_product(normed, both_ref[...]).astype(out_ref.dtype)
    out_ref[:, LANES : 2 * LANES] = jnp.dot(
        normed, value_ref[...], preferred_element_type=jnp.float32
    ).astype(out_ref.dtype)
    out_ref[:, 2 * LANES : 3 * LANES] = jnp.dot(
        normed, ogate_ref[...], preferred_element_type=jnp.float32
    ).astype(out_ref.dtype)
    wide = normed.astype(jnp.float32)
    squares = jnp.sum(x * x, axis=1, keepdims=True)
    igate = jnp.sum(wide * vectors_ref[1:2, :], axis=1, keepdims=True)
    fgate = jnp.sum(wide * vectors_ref[2:3, :], axis=1, keepdims=True)
    lane = lax.broadcasted_iota(jnp.int32, (x.shape[0], LANES), 1)
    tail = jnp.where(
        lane == 0, igate, jnp.where(lane == 1, fgate, jnp.where(lane == 2, squares, 0.0))
    )
    own = (small_ref.shape[0] - 3) // 2
    gain_tile = small_ref[own : 2 * own, :]
    tail += jnp.concatenate([gain_tile] * (x.shape[0] // own), axis=0)
    out_ref[:, 3 * LANES :] = tail.astype(out_ref.dtype)


def project(x, vectors, small, w_both, w_value, w_ogate):
    return pl.pallas_call(
        project_kernel,
        out_shape=(
            jax.ShapeDtypeStruct((x.shape[1], 4 * LANES), jnp.bfloat16),
            jax.ShapeDtypeStruct(small.shape, small.dtype),
        ),
        in_specs=[VMEM] * 6,
        out_specs=(VMEM, VMEM),
        compiler_params=SMALL,
        name="project",
    )(x, vectors, small, w_both, w_value, w_ogate)


def cell_kernel(
    parts_ref, c_ref, small_ref,
    new_c_ref, new_n_ref, new_m_ref, other_ref, out_ref,
):
    total = parts_ref[0].astype(jnp.float32)
    for k in range(1, parts_ref.shape[0]):
        total += parts_ref[k].astype(jnp.float32)
    seqs = total.shape[0]
    tail = total[:, 3 * LANES :]
    row_scale = lax.rsqrt(tail[:, 2:3] / D + norm_eps)
    igate = igate_cap * jnp.tanh((row_scale * tail[:, 0:1] + small_ref[2 * seqs + 2 : 2 * seqs + 3, 0:1]) / igate_cap)
    fgate = row_scale * tail[:, 1:2] + small_ref[2 * seqs + 2 : 2 * seqs + 3, 1:2]
    diagonal = lax.broadcasted_iota(jnp.int32, (seqs, seqs), 0) == lax.broadcasted_iota(
        jnp.int32, (seqs, seqs), 1
    )
    state_m = jnp.sum(jnp.where(diagonal, small_ref[2 * seqs : 2 * seqs + 1, :seqs], 0.0), axis=1, keepdims=True)
    log_keep = jnp.minimum(fgate, 0.0) - jnp.log1p(jnp.exp(-jnp.abs(fgate)))
    carried = log_keep + state_m
    new_m = jnp.maximum(carried, igate)
    keep = jnp.exp(carried - new_m)
    write = jnp.exp(igate - new_m)
    new_m_ref[...] = jnp.sum(jnp.where(diagonal, new_m, 0.0), axis=0, keepdims=True)
    lane = lax.broadcasted_iota(jnp.int32, (seqs, LANES), 1)
    first = total[:, :LANES]
    query_key = row_scale * jnp.where(lane < DK, first, first * DK ** (-0.5))
    query = query_key[:, :DK]
    key_vec = query_key[:, DK:]
    value_vec = row_scale * total[:, LANES : 2 * LANES]
    ogate = row_scale * total[:, 2 * LANES : 3 * LANES]
    new_n = keep * small_ref[:seqs, :DK] + write * key_vec
    new_n_ref[...] = new_n
    denominator = jnp.maximum(
        jnp.abs(jnp.sum(query * new_n, axis=1, keepdims=True)), jnp.exp(-new_m)
    )
    columns = jnp.where(lane < DK, query_key, write * query_key).T
    rows = []
    for b in range(seqs):
        query_b = columns[:DK, b : b + 1]
        key_b = columns[DK:, b : b + 1]
        new_c = keep[b : b + 1, :] * c_ref[b] + key_b * value_vec[b : b + 1, :]
        new_c_ref[b] = new_c
        rows.append(jnp.sum(query_b * new_c, axis=0, keepdims=True))
    me = lax.axis_index("kv")
    theirs = parts_ref[pl.ds(me + 1 - 2 * lax.rem(me, 2), 1)][0]
    theirs = theirs[:, 3 * LANES :].astype(jnp.float32)
    start, share = LANES // 2, other_ref.shape[1] // seqs
    other_ref[...] = jnp.concatenate(
        [theirs[b : b + 1, start : start + share] for b in range(seqs)], axis=1
    )
    head_out = jnp.concatenate(rows, axis=0) / denominator
    merged = head_out * small_ref[2 * seqs + 1 : 2 * seqs + 2, :] / (1.0 + jnp.exp(-ogate))
    merged = merged.astype(out_ref.dtype)
    for copy in range(out_ref.shape[0]):
        out_ref[copy] = merged


def cell(parts, state_c, small, width):
    count, seqs, _ = parts.shape
    *states, other, out = pl.pallas_call(
        cell_kernel,
        out_shape=(
            jax.ShapeDtypeStruct((seqs, DK, DV), jnp.float32),
            jax.ShapeDtypeStruct((seqs, DK), jnp.float32),
            jax.ShapeDtypeStruct((1, seqs), jnp.float32),
            jax.ShapeDtypeStruct((1, width), jnp.float32),
            jax.ShapeDtypeStruct((count, seqs, DV), jnp.bfloat16),
        ),
        in_specs=[VMEM] * 3,
        out_specs=(VMEM,) * 5,
        compiler_params=SMALL,
        name="cell",
    )(
        parts, state_c.reshape(seqs, DK, DV), small,
    )
    return states, other, out


def residual_kernel(parts_ref, tokens_ref, own_ref, out_ref):
    total = parts_ref[0].astype(jnp.float32)
    for k in range(1, parts_ref.shape[0]):
        total += parts_ref[k].astype(jnp.float32)
    middle = (tokens_ref[...].astype(jnp.float32) + total).astype(own_ref.dtype)
    own_ref[...] = middle
    middle = middle.astype(jnp.float32)
    feats, seqs = middle.shape
    copies = out_ref.shape[0] // 2
    for half in range(2):
        at = half * (seqs // 2)
        picked = middle[:, at : at + seqs // 2]
        packed = jnp.concatenate([picked[: feats // 2], picked[feats // 2 :]], axis=1)
        packed = packed.astype(out_ref.dtype)
        for copy in range(copies):
            out_ref[half * copies + copy] = packed


def residual(parts, tokens):
    count, feats, seqs = parts.shape
    return pl.pallas_call(
        residual_kernel,
        out_shape=(
            jax.ShapeDtypeStruct((feats, seqs), parts.dtype),
            jax.ShapeDtypeStruct((2 * count, feats // 2, seqs), parts.dtype),
        ),
        in_specs=[VMEM, VMEM],
        out_specs=(VMEM, VMEM),
        compiler_params=SMALL,
        name="residual",
    )(parts, tokens)


def finish_kernel(parts_ref, middle_ref, *refs):
    count = (len(refs) - 3) // 2
    states, out_ref, targets = refs[:count], refs[count], refs[count + 1 : -2]
    tokens, sems = refs[-2:]
    copies = [
        pltpu.make_async_copy(state, target, sems.at[k])
        for k, (state, target) in enumerate(zip(states, targets))
    ]
    for copy in copies:
        copy.start()
    total = parts_ref[0].astype(jnp.float32)
    for k in range(1, parts_ref.shape[0]):
        total += parts_ref[k].astype(jnp.float32)
    tokens[...] = (middle_ref[...].astype(jnp.float32) + total).astype(tokens.dtype)
    copies.append(pltpu.make_async_copy(tokens, out_ref, sems.at[count]))
    copies[count].start()
    for copy in copies:
        copy.wait()


def finish(parts, middle, *states):
    return pl.pallas_call(
        finish_kernel,
        out_shape=(
            jax.ShapeDtypeStruct(parts.shape[1:], parts.dtype),
            *(jax.ShapeDtypeStruct(one.shape, one.dtype) for one in states),
        ),
        in_specs=[VMEM] * (2 + len(states)),
        out_specs=(ANY,) * (1 + len(states)),
        scratch_shapes=[
            pltpu.VMEM(parts.shape[1:], parts.dtype),
            pltpu.SemaphoreType.DMA((1 + len(states),)),
        ],
        compiler_params=SMALL,
        name="finish",
    )(parts, middle, *states)


def widen_kernel(
    x_ref, vectors_ref, gain_ref, gate_ref, up_ref, other_gate_ref, other_up_ref, out_ref
):
    blocks = x_ref.shape[0] // 2
    half = x_ref.shape[2] // 2
    units = gate_ref.shape[0]
    cols = out_ref.shape[1]
    start = units // LANES * LANES
    taken = (LANES - (units - start)) % LANES
    place = lax.rem(lax.axis_index("kv"), 2)

    def features(which):
        packed = x_ref[pl.ds(which * blocks, blocks)].astype(jnp.float32)
        both = jnp.concatenate([packed[:, :, :half], packed[:, :, half:]], axis=1)
        return both.reshape(-1, half).T

    own, other = features(place), features(1 - place)
    squares = jnp.sum(own * own, axis=1, keepdims=True) + jnp.sum(
        other * other, axis=1, keepdims=True
    )
    own = (own * vectors_ref[3:4, :]).astype(jnp.bfloat16)
    other = (other * gain_ref[...]).astype(jnp.bfloat16)

    def product(pick):
        return transposed_product(own, pick(gate_ref, up_ref)) + transposed_product(
            other, pick(other_gate_ref, other_up_ref)
        )

    out_ref[:, :start] = product(lambda gate, up: gate[:start, :]).astype(out_ref.dtype)
    if taken:
        mixed = product(
            lambda gate, up: jnp.concatenate([gate[start:, :], up[:taken, :]], axis=0)
        )
        out_ref[:, start : start + LANES] = mixed.astype(out_ref.dtype)
        start += LANES
    filler = jnp.zeros((cols - 2 * units, gate_ref.shape[1]), gate_ref.dtype)
    rest = product(lambda gate, up: jnp.concatenate([up[taken:, :], filler], axis=0))
    lane = lax.broadcasted_iota(jnp.int32, rest.shape, 1)
    out_ref[:, start:] = jnp.where(lane == 2 * units - start, squares, rest).astype(out_ref.dtype)


def widen(x, vectors, other_gain, *weights):
    cols = (2 * weights[0].shape[0] // LANES + 1) * LANES
    return pl.pallas_call(
        widen_kernel,
        out_shape=jax.ShapeDtypeStruct((x.shape[2] // 2, cols), jnp.bfloat16),
        in_specs=[VMEM] * 7,
        out_specs=VMEM,
        compiler_params=SMALL,
        name="widen",
    )(x, vectors, other_gain, *weights)


def body(
    tokens,
    norm_gain,
    w_query,
    w_key,
    w_value,
    w_ogate,
    w_igate,
    w_fgate,
    igate_bias,
    fgate_bias,
    state_c,
    state_n,
    state_m,
    head_gain,
    w_out,
    ffn_gain,
    w_gate,
    w_up,
    w_down,
):
    n_kv, n_tp = lax.axis_size("kv"), lax.axis_size("tp")
    seqs, feats = tokens.shape
    units = w_gate.shape[1]
    rows = n_tp * feats
    own_seqs = seqs // n_kv

    wide = [norm_gain[None], w_igate.T, w_fgate.T, ffn_gain[None]]
    vectors = jnp.concatenate(wide, axis=0).astype(jnp.float32)
    narrow = [
        state_n.reshape(own_seqs, DK), state_m.T, head_gain.astype(jnp.float32),
        jnp.stack([igate_bias, fgate_bias], axis=1),
    ]
    narrow = [jnp.pad(one, ((0, 0), (0, LANES - one.shape[1]))) for one in narrow]
    share = rows // own_seqs
    gain_tile = jnp.pad(
        ffn_gain.astype(jnp.float32).reshape(own_seqs, share),
        ((0, 0), (LANES // 2, LANES // 2 - share)),
    )
    small = jnp.concatenate([narrow[0], gain_tile, *narrow[1:]], axis=0)
    token_copies, own_tokens = spread(tokens.T, n_tp)
    token_rows = exchanged(token_copies, "tp").reshape(rows, seqs)
    w_both = jnp.concatenate([w_query.T, w_key.T], axis=0)
    parts, small = project(token_rows, vectors, small, w_both, w_value, w_ogate)
    arrived = exchanged(parts.reshape(n_kv, own_seqs, -1), "kv")
    states, other_gain, merged = cell(arrived, state_c, small, rows)
    merged_all = exchanged(merged, "kv").reshape(seqs, -1)
    gate, up = w_gate.T, w_up.T
    merged_all, sent_gate, sent_up = lax.optimization_barrier((merged_all, gate, up))
    swap = [(k, k + 1 - 2 * (k % 2)) for k in range(n_kv)]
    other_gate = lax.ppermute(sent_gate, "kv", swap)
    other_up = lax.ppermute(sent_up, "kv", swap)
    attn_part = jnp.dot(merged_all, w_out, preferred_element_type=jnp.float32)
    attn_part = attn_part.astype(jnp.bfloat16).T.reshape(n_tp, feats, seqs)
    own_middle, middle_copies = residual(exchanged(attn_part, "tp"), own_tokens)
    pairs = [[k * n_tp + t for t in range(2 * n_tp)] for k in range(0, n_kv, 2)]
    middle_rows = exchanged(middle_copies, ("kv", "tp"), pairs)
    partial = widen(middle_rows, vectors, other_gain, gate, up, other_gate, other_up)
    halves = [list(range(place, n_kv, 2)) for place in range(2)]
    arrived = exchanged(partial.reshape(n_kv // 2, own_seqs, -1), "kv", halves)
    sums = arrived.astype(jnp.float32).sum(axis=0)
    gate_sum, up_sum, total = sums[:, :units], sums[:, units : 2 * units], sums[:, 2 * units]
    ffn_scale = lax.rsqrt(total / D + norm_eps)[:, None]
    hidden = (jax.nn.silu(ffn_scale * gate_sum) * (ffn_scale * up_sum)).astype(jnp.bfloat16)
    hidden_all = exchanged(
        jnp.broadcast_to(hidden[None], (n_kv, *hidden.shape)), "kv", [halves[0] + halves[1]]
    ).reshape(seqs, units)
    down_part = jnp.dot(hidden_all, w_down, preferred_element_type=jnp.float32)
    down_part = down_part.astype(jnp.bfloat16).T.reshape(n_tp, feats, seqs)
    out_tokens, new_c, new_n, new_m = finish(
        exchanged(down_part, "tp"), own_middle, *states
    )
    new_n = new_n.reshape(own_seqs, 1, DK)
    return (out_tokens.T, new_c.reshape(state_c.shape), new_n, new_m.T)


def solution(mesh):
    placed = (
        P("grp", ("kv", "tp")),
        P("kv"),
        P("kv", "tp"),
        P("kv", "tp"),
        P("kv", "tp"),
        P("kv", "tp"),
        P("kv", "tp"),
        P("kv", "tp"),
        P("tp"),
        P("tp"),
        P(("grp", "kv"), "tp", None, None),
        P(("grp", "kv"), "tp", None),
        P(("grp", "kv"), "tp"),
        P("tp", None),
        P("tp", "kv"),
        P("kv"),
        P("kv", "tp"),
        P("kv", "tp"),
        P("tp", "kv"),
    )
    return jax.shard_map(
        body,
        mesh=mesh,
        in_specs=placed,
        out_specs=(
            P("grp", ("kv", "tp")),
            P(("grp", "kv"), "tp", None, None),
            P(("grp", "kv"), "tp", None),
            P(("grp", "kv"), "tp"),
        ),
        check_vma=False,
    )
```

```python
import functools

import jax
import jax.numpy as jnp
from jax import lax
from jax.experimental import pallas as pl
from jax.experimental.pallas import tpu as pltpu
from jax.sharding import PartitionSpec as P

D = 4096
DK = 64
DV = 128
LANES = 128


norm_eps = 1e-06
igate_cap = 1.5

VMEM = pl.BlockSpec(memory_space=pltpu.VMEM)
ANY = pl.BlockSpec(memory_space=pl.ANY)
SMALL = pltpu.CompilerParams(vmem_limit_bytes=8 * 2**20)


def exchanged(blocks, axis, groups=None):
    return lax.all_to_all(
        blocks, axis, split_axis=0, concat_axis=0, tiled=True, axis_index_groups=groups
    )


def spread_kernel(value_ref, out_ref, own_ref):
    value = value_ref[...]
    own_ref[...] = value
    for copy in range(out_ref.shape[0]):
        out_ref[copy] = value


def spread(value, count):
    return pl.pallas_call(
        spread_kernel,
        out_shape=(
            jax.ShapeDtypeStruct((count, *value.shape), value.dtype),
            jax.ShapeDtypeStruct(value.shape, value.dtype),
        ),
        in_specs=[VMEM],
        out_specs=(VMEM, VMEM),
        compiler_params=SMALL,
        name="spread",
    )(value)


def transposed_product(x, weight):
    return lax.dot_general(
        x, weight, (((1,), (1,)), ((), ())), preferred_element_type=jnp.float32
    )


def project_kernel(
    x_ref, vectors_ref, small_ref, both_ref, value_ref, ogate_ref, out_ref, handed_ref
):
    handed_ref[...] = small_ref[...]
    x = x_ref[...].astype(jnp.float32).T
    normed = (x * vectors_ref[0:1, :]).astype(jnp.bfloat16)
    out_ref[:, :LANES] = transposed_product(normed, both_ref[...]).astype(out_ref.dtype)
    out_ref[:, LANES : 2 * LANES] = jnp.dot(
        normed, value_ref[...], preferred_element_type=jnp.float32
    ).astype(out_ref.dtype)
    out_ref[:, 2 * LANES : 3 * LANES] = jnp.dot(
        normed, ogate_ref[...], preferred_element_type=jnp.float32
    ).astype(out_ref.dtype)
    wide = normed.astype(jnp.float32)
    squares = jnp.sum(x * x, axis=1, keepdims=True)
    igate = jnp.sum(wide * vectors_ref[1:2, :], axis=1, keepdims=True)
    fgate = jnp.sum(wide * vectors_ref[2:3, :], axis=1, keepdims=True)
    lane = lax.broadcasted_iota(jnp.int32, (x.shape[0], LANES), 1)
    tail = jnp.where(
        lane == 0, igate, jnp.where(lane == 1, fgate, jnp.where(lane == 2, squares, 0.0))
    )
    own = (small_ref.shape[0] - 3) // 2
    gain_tile = small_ref[own : 2 * own, :]
    tail += jnp.concatenate([gain_tile] * (x.shape[0] // own), axis=0)
    out_ref[:, 3 * LANES :] = tail.astype(out_ref.dtype)


def project(x, vectors, small, w_both, w_value, w_ogate):
    return pl.pallas_call(
        project_kernel,
        out_shape=(
            jax.ShapeDtypeStruct((x.shape[1], 4 * LANES), jnp.bfloat16),
            jax.ShapeDtypeStruct(small.shape, small.dtype),
        ),
        in_specs=[VMEM] * 6,
        out_specs=(VMEM, VMEM),
        compiler_params=SMALL,
        name="project",
    )(x, vectors, small, w_both, w_value, w_ogate)


def cell_kernel(
    parts_ref, c_ref, small_ref,
    new_c_ref, new_n_ref, new_m_ref, other_ref, out_ref,
):
    total = parts_ref[0].astype(jnp.float32)
    for k in range(1, parts_ref.shape[0]):
        total += parts_ref[k].astype(jnp.float32)
    seqs = total.shape[0]
    tail = total[:, 3 * LANES :]
    row_scale = lax.rsqrt(tail[:, 2:3] / D + norm_eps)
    igate = igate_cap * jnp.tanh((row_scale * tail[:, 0:1] + small_ref[2 * seqs + 2 : 2 * seqs + 3, 0:1]) / igate_cap)
    fgate = row_scale * tail[:, 1:2] + small_ref[2 * seqs + 2 : 2 * seqs + 3, 1:2]
    diagonal = lax.broadcasted_iota(jnp.int32, (seqs, seqs), 0) == lax.broadcasted_iota(
        jnp.int32, (seqs, seqs), 1
    )
    state_m = jnp.sum(jnp.where(diagonal, small_ref[2 * seqs : 2 * seqs + 1, :seqs], 0.0), axis=1, keepdims=True)
    log_keep = jnp.minimum(fgate, 0.0) - jnp.log1p(jnp.exp(-jnp.abs(fgate)))
    carried = log_keep + state_m
    new_m = jnp.maximum(carried, igate)
    keep = jnp.exp(carried - new_m)
    write = jnp.exp(igate - new_m)
    new_m_ref[...] = jnp.sum(jnp.where(diagonal, new_m, 0.0), axis=0, keepdims=True)
    lane = lax.broadcasted_iota(jnp.int32, (seqs, LANES), 1)
    first = total[:, :LANES]
    query_key = row_scale * jnp.where(lane < DK, first, first * DK ** (-0.5))
    query = query_key[:, :DK]
    key_vec = query_key[:, DK:]
    value_vec = row_scale * total[:, LANES : 2 * LANES]
    ogate = row_scale * total[:, 2 * LANES : 3 * LANES]
    new_n = keep * small_ref[:seqs, :DK] + write * key_vec
    new_n_ref[...] = new_n
    denominator = jnp.maximum(
        jnp.abs(jnp.sum(query * new_n, axis=1, keepdims=True)), jnp.exp(-new_m)
    )
    columns = jnp.where(lane < DK, query_key, write * query_key).T
    rows = []
    for b in range(seqs):
        query_b = columns[:DK, b : b + 1]
        key_b = columns[DK:, b : b + 1]
        new_c = keep[b : b + 1, :] * c_ref[b] + key_b * value_vec[b : b + 1, :]
        new_c_ref[b] = new_c
        rows.append(jnp.sum(query_b * new_c, axis=0, keepdims=True))
    me = lax.axis_index("kv")
    theirs = parts_ref[pl.ds(me + 1 - 2 * lax.rem(me, 2), 1)][0]
    theirs = theirs[:, 3 * LANES :].astype(jnp.float32)
    start, share = LANES // 2, other_ref.shape[1] // seqs
    other_ref[...] = jnp.concatenate(
        [theirs[b : b + 1, start : start + share] for b in range(seqs)], axis=1
    )
    head_out = jnp.concatenate(rows, axis=0) / denominator
    merged = head_out * small_ref[2 * seqs + 1 : 2 * seqs + 2, :] / (1.0 + jnp.exp(-ogate))
    merged = merged.astype(out_ref.dtype)
    for place in range(out_ref.shape[0]):
        out_ref[place] = merged


def cell(parts, state_c, small, width):
    count, seqs, _ = parts.shape
    *states, other, out = pl.pallas_call(
        cell_kernel,
        out_shape=(
            jax.ShapeDtypeStruct((seqs, DK, DV), jnp.float32),
            jax.ShapeDtypeStruct((seqs, DK), jnp.float32),
            jax.ShapeDtypeStruct((1, seqs), jnp.float32),
            jax.ShapeDtypeStruct((1, width), jnp.float32),
            jax.ShapeDtypeStruct((count, seqs, DV), jnp.bfloat16),
        ),
        in_specs=[VMEM] * 3,
        out_specs=(VMEM,) * 5,
        compiler_params=SMALL,
        name="cell",
    )(
        parts, state_c.reshape(seqs, DK, DV), small,
    )
    return states, other, out


def residual_kernel(parts_ref, tokens_ref, own_ref, out_ref):
    total = parts_ref[0].astype(jnp.float32)
    for k in range(1, parts_ref.shape[0]):
        total += parts_ref[k].astype(jnp.float32)
    middle = (tokens_ref[...].astype(jnp.float32) + total).astype(own_ref.dtype)
    own_ref[...] = middle
    middle = middle.astype(jnp.float32)
    feats, seqs = middle.shape
    copies = out_ref.shape[0] // 2
    for half in range(2):
        at = half * (seqs // 2)
        picked = middle[:, at : at + seqs // 2]
        packed = jnp.concatenate([picked[: feats // 2], picked[feats // 2 :]], axis=1)
        packed = packed.astype(out_ref.dtype)
        for copy in range(copies):
            out_ref[half * copies + copy] = packed


def residual(parts, tokens):
    count, feats, seqs = parts.shape
    return pl.pallas_call(
        residual_kernel,
        out_shape=(
            jax.ShapeDtypeStruct((feats, seqs), parts.dtype),
            jax.ShapeDtypeStruct((2 * count, feats // 2, seqs), parts.dtype),
        ),
        in_specs=[VMEM, VMEM],
        out_specs=(VMEM, VMEM),
        compiler_params=SMALL,
        name="residual",
    )(parts, tokens)


def finish_kernel(parts_ref, middle_ref, *refs):
    count = (len(refs) - 3) // 2
    states, out_ref, targets = refs[:count], refs[count], refs[count + 1 : -2]
    tokens, sems = refs[-2:]
    copies = [
        pltpu.make_async_copy(state, target, sems.at[k])
        for k, (state, target) in enumerate(zip(states, targets))
    ]
    for copy in copies:
        copy.start()
    total = parts_ref[0].astype(jnp.float32)
    for k in range(1, parts_ref.shape[0]):
        total += parts_ref[k].astype(jnp.float32)
    tokens[...] = (middle_ref[...].astype(jnp.float32) + total).astype(tokens.dtype)
    copies.append(pltpu.make_async_copy(tokens, out_ref, sems.at[count]))
    copies[count].start()
    for copy in copies:
        copy.wait()


def finish(parts, middle, *states):
    return pl.pallas_call(
        finish_kernel,
        out_shape=(
            jax.ShapeDtypeStruct(parts.shape[1:], parts.dtype),
            *(jax.ShapeDtypeStruct(one.shape, one.dtype) for one in states),
        ),
        in_specs=[VMEM] * (2 + len(states)),
        out_specs=(ANY,) * (1 + len(states)),
        scratch_shapes=[
            pltpu.VMEM(parts.shape[1:], parts.dtype),
            pltpu.SemaphoreType.DMA((1 + len(states),)),
        ],
        compiler_params=SMALL,
        name="finish",
    )(parts, middle, *states)


def pack_kernel(gate_ref, up_ref, out_ref, sems):
    units = gate_ref.shape[0]
    copies = [
        pltpu.make_async_copy(source, out_ref.at[pl.ds(k * units, units)], sems.at[k])
        for k, source in enumerate((gate_ref, up_ref))
    ]
    for copy in copies:
        copy.start()
    for copy in copies:
        copy.wait()


def pack(gate, up):
    units, rows = gate.shape
    return pl.pallas_call(
        pack_kernel,
        out_shape=jax.ShapeDtypeStruct((2 * units, rows), gate.dtype),
        in_specs=[ANY, ANY],
        out_specs=VMEM,
        scratch_shapes=[pltpu.SemaphoreType.DMA((2,))],
        compiler_params=SMALL,
        name="pack",
    )(gate, up)


def widen_kernel(x_ref, vectors_ref, gain_ref, own_ref, other_ref, out_ref):
    blocks = x_ref.shape[0] // 2
    half = x_ref.shape[2] // 2
    units = own_ref.shape[0]
    cols = out_ref.shape[1]
    last = cols - LANES
    place = lax.rem(lax.axis_index("kv"), 2)

    def features(which):
        packed = x_ref[pl.ds(which * blocks, blocks)].astype(jnp.float32)
        both = jnp.concatenate([packed[:, :, :half], packed[:, :, half:]], axis=1)
        return both.reshape(-1, half).T

    own, other = features(place), features(1 - place)
    squares = jnp.sum(own * own, axis=1, keepdims=True) + jnp.sum(
        other * other, axis=1, keepdims=True
    )
    own = (own * vectors_ref[3:4, :]).astype(jnp.bfloat16)
    other = (other * gain_ref[...]).astype(jnp.bfloat16)
    out_ref[:, :last] = (
        transposed_product(own, own_ref[:last, :]) + transposed_product(other, other_ref[:last, :])
    ).astype(out_ref.dtype)
    filler = jnp.zeros((cols - units, own_ref.shape[1]), own_ref.dtype)
    rest = transposed_product(
        own, jnp.concatenate([own_ref[last:, :], filler], axis=0)
    ) + transposed_product(other, jnp.concatenate([other_ref[last:, :], filler], axis=0))
    lane = lax.broadcasted_iota(jnp.int32, rest.shape, 1)
    out_ref[:, last:] = jnp.where(lane == units - last, squares, rest).astype(out_ref.dtype)


def widen(x, vectors, other_gain, own, other):
    cols = (own.shape[0] // LANES + 1) * LANES
    return pl.pallas_call(
        widen_kernel,
        out_shape=jax.ShapeDtypeStruct((x.shape[2] // 2, cols), jnp.bfloat16),
        in_specs=[VMEM] * 5,
        out_specs=VMEM,
        compiler_params=SMALL,
        name="widen",
    )(x, vectors, other_gain, own, other)


def body(
    tokens,
    norm_gain,
    w_query,
    w_key,
    w_value,
    w_ogate,
    w_igate,
    w_fgate,
    igate_bias,
    fgate_bias,
    state_c,
    state_n,
    state_m,
    head_gain,
    w_out,
    ffn_gain,
    w_gate,
    w_up,
    w_down,
):
    n_kv, n_tp = lax.axis_size("kv"), lax.axis_size("tp")
    seqs, feats = tokens.shape
    units = w_gate.shape[1]
    rows = n_tp * feats
    own_seqs = seqs // n_kv

    wide = [norm_gain[None], w_igate.T, w_fgate.T, ffn_gain[None]]
    vectors = jnp.concatenate(wide, axis=0).astype(jnp.float32)
    narrow = [
        state_n.reshape(own_seqs, DK), state_m.T, head_gain.astype(jnp.float32),
        jnp.stack([igate_bias, fgate_bias], axis=1),
    ]
    narrow = [jnp.pad(one, ((0, 0), (0, LANES - one.shape[1]))) for one in narrow]
    share = rows // own_seqs
    gain_tile = jnp.pad(
        ffn_gain.astype(jnp.float32).reshape(own_seqs, share),
        ((0, 0), (LANES // 2, LANES // 2 - share)),
    )
    small = jnp.concatenate([narrow[0], gain_tile, *narrow[1:]], axis=0)
    token_copies, own_tokens = spread(tokens.T, n_tp)
    token_rows = exchanged(token_copies, "tp").reshape(rows, seqs)
    w_both = jnp.concatenate([w_query.T, w_key.T], axis=0)
    parts, small = project(token_rows, vectors, small, w_both, w_value, w_ogate)
    arrived = exchanged(parts.reshape(n_kv, own_seqs, -1), "kv")
    states, other_gain, merged = cell(arrived, state_c, small, rows)
    merged_all = exchanged(merged, "kv").reshape(seqs, -1)
    merged_all, gate, up = lax.optimization_barrier((merged_all, w_gate.T, w_up.T))
    own_weights = pack(gate, up)
    swap = [(k, k + 1 - 2 * (k % 2)) for k in range(n_kv)]
    other_weights = lax.ppermute(own_weights, "kv", swap)
    attn_part = jnp.dot(merged_all, w_out, preferred_element_type=jnp.float32)
    attn_part = attn_part.astype(jnp.bfloat16).T.reshape(n_tp, feats, seqs)
    own_middle, middle_copies = residual(exchanged(attn_part, "tp"), own_tokens)
    pairs = [[k * n_tp + t for t in range(2 * n_tp)] for k in range(0, n_kv, 2)]
    middle_rows = exchanged(middle_copies, ("kv", "tp"), pairs)
    partial = widen(middle_rows, vectors, other_gain, own_weights, other_weights)
    halves = [list(range(place, n_kv, 2)) for place in range(2)]
    arrived = exchanged(partial.reshape(n_kv // 2, own_seqs, -1), "kv", halves)
    sums = arrived.astype(jnp.float32).sum(axis=0)
    gate_sum, up_sum, total = sums[:, :units], sums[:, units : 2 * units], sums[:, 2 * units]
    ffn_scale = lax.rsqrt(total / D + norm_eps)[:, None]
    hidden = (jax.nn.silu(ffn_scale * gate_sum) * (ffn_scale * up_sum)).astype(jnp.bfloat16)
    hidden_all = exchanged(
        jnp.broadcast_to(hidden[None], (n_kv, *hidden.shape)), "kv", [halves[0] + halves[1]]
    ).reshape(seqs, units)
    down_part = jnp.dot(hidden_all, w_down, preferred_element_type=jnp.float32)
    down_part = down_part.astype(jnp.bfloat16).T.reshape(n_tp, feats, seqs)
    out_tokens, new_c, new_n, new_m = finish(
        exchanged(down_part, "tp"), own_middle, *states
    )
    new_n = new_n.reshape(own_seqs, 1, DK)
    return (out_tokens.T, new_c.reshape(state_c.shape), new_n, new_m.T)


def solution(mesh):
    placed = (
        P("grp", ("kv", "tp")),
        P("kv"),
        P("kv", "tp"),
        P("kv", "tp"),
        P("kv", "tp"),
        P("kv", "tp"),
        P("kv", "tp"),
        P("kv", "tp"),
        P("tp"),
        P("tp"),
        P(("grp", "kv"), "tp", None, None),
        P(("grp", "kv"), "tp", None),
        P(("grp", "kv"), "tp"),
        P("tp", None),
        P("tp", "kv"),
        P("kv"),
        P("kv", "tp"),
        P("kv", "tp"),
        P("tp", "kv"),
    )
    return jax.shard_map(
        body,
        mesh=mesh,
        in_specs=placed,
        out_specs=(
            P("grp", ("kv", "tp")),
            P(("grp", "kv"), "tp", None, None),
            P(("grp", "kv"), "tp", None),
            P(("grp", "kv"), "tp"),
        ),
        check_vma=False,
    )
```

```python
import functools

import jax
import jax.numpy as jnp
from jax import lax
from jax.experimental import pallas as pl
from jax.experimental.pallas import tpu as pltpu
from jax.sharding import PartitionSpec as P

D = 4096
DK = 64
DV = 128
LANES = 128


norm_eps = 1e-06
igate_cap = 1.5

VMEM = pl.BlockSpec(memory_space=pltpu.VMEM)
ANY = pl.BlockSpec(memory_space=pl.ANY)
SMALL = pltpu.CompilerParams(vmem_limit_bytes=8 * 2**20)


def exchanged(blocks, axis, groups=None):
    return lax.all_to_all(
        blocks, axis, split_axis=0, concat_axis=0, tiled=True, axis_index_groups=groups
    )


def spread_kernel(value_ref, out_ref, own_ref):
    value = value_ref[...]
    own_ref[...] = value
    for copy in range(out_ref.shape[0]):
        out_ref[copy] = value


def spread(value, count):
    return pl.pallas_call(
        spread_kernel,
        out_shape=(
            jax.ShapeDtypeStruct((count, *value.shape), value.dtype),
            jax.ShapeDtypeStruct(value.shape, value.dtype),
        ),
        in_specs=[VMEM],
        out_specs=(VMEM, VMEM),
        compiler_params=SMALL,
        name="spread",
    )(value)


def transposed_product(x, weight):
    return lax.dot_general(
        x, weight, (((1,), (1,)), ((), ())), preferred_element_type=jnp.float32
    )


def project_kernel(
    x_ref, vectors_ref, small_ref, both_ref, value_ref, ogate_ref, out_ref, handed_ref
):
    handed_ref[...] = small_ref[...]
    x = x_ref[...].astype(jnp.float32).T
    normed = (x * vectors_ref[0:1, :]).astype(jnp.bfloat16)
    out_ref[:, :LANES] = transposed_product(normed, both_ref[...]).astype(out_ref.dtype)
    out_ref[:, LANES : 2 * LANES] = jnp.dot(
        normed, value_ref[...], preferred_element_type=jnp.float32
    ).astype(out_ref.dtype)
    out_ref[:, 2 * LANES : 3 * LANES] = jnp.dot(
        normed, ogate_ref[...], preferred_element_type=jnp.float32
    ).astype(out_ref.dtype)
    wide = normed.astype(jnp.float32)
    squares = jnp.sum(x * x, axis=1, keepdims=True)
    igate = jnp.sum(wide * vectors_ref[1:2, :], axis=1, keepdims=True)
    fgate = jnp.sum(wide * vectors_ref[2:3, :], axis=1, keepdims=True)
    lane = lax.broadcasted_iota(jnp.int32, (x.shape[0], LANES), 1)
    tail = jnp.where(
        lane == 0, igate, jnp.where(lane == 1, fgate, jnp.where(lane == 2, squares, 0.0))
    )
    own = (small_ref.shape[0] - 3) // 2
    gain_tile = small_ref[own : 2 * own, :]
    tail += jnp.concatenate([gain_tile] * (x.shape[0] // own), axis=0)
    out_ref[:, 3 * LANES :] = tail.astype(out_ref.dtype)


def project(x, vectors, small, w_both, w_value, w_ogate):
    return pl.pallas_call(
        project_kernel,
        out_shape=(
            jax.ShapeDtypeStruct((x.shape[1], 4 * LANES), jnp.bfloat16),
            jax.ShapeDtypeStruct(small.shape, small.dtype),
        ),
        in_specs=[VMEM] * 6,
        out_specs=(VMEM, VMEM),
        compiler_params=SMALL,
        name="project",
    )(x, vectors, small, w_both, w_value, w_ogate)


def cell_kernel(
    parts_ref, c_ref, small_ref,
    new_c_ref, new_n_ref, new_m_ref, other_ref, out_ref,
):
    total = parts_ref[0].astype(jnp.float32)
    for k in range(1, parts_ref.shape[0]):
        total += parts_ref[k].astype(jnp.float32)
    seqs = total.shape[0]
    tail = total[:, 3 * LANES :]
    row_scale = lax.rsqrt(tail[:, 2:3] / D + norm_eps)
    igate = igate_cap * jnp.tanh((row_scale * tail[:, 0:1] + small_ref[2 * seqs + 2 : 2 * seqs + 3, 0:1]) / igate_cap)
    fgate = row_scale * tail[:, 1:2] + small_ref[2 * seqs + 2 : 2 * seqs + 3, 1:2]
    diagonal = lax.broadcasted_iota(jnp.int32, (seqs, seqs), 0) == lax.broadcasted_iota(
        jnp.int32, (seqs, seqs), 1
    )
    state_m = jnp.sum(jnp.where(diagonal, small_ref[2 * seqs : 2 * seqs + 1, :seqs], 0.0), axis=1, keepdims=True)
    log_keep = jnp.minimum(fgate, 0.0) - jnp.log1p(jnp.exp(-jnp.abs(fgate)))
    carried = log_keep + state_m
    new_m = jnp.maximum(carried, igate)
    keep = jnp.exp(carried - new_m)
    write = jnp.exp(igate - new_m)
    new_m_ref[...] = jnp.sum(jnp.where(diagonal, new_m, 0.0), axis=0, keepdims=True)
    lane = lax.broadcasted_iota(jnp.int32, (seqs, LANES), 1)
    first = total[:, :LANES]
    query_key = row_scale * jnp.where(lane < DK, first, first * DK ** (-0.5))
    query = query_key[:, :DK]
    key_vec = query_key[:, DK:]
    value_vec = row_scale * total[:, LANES : 2 * LANES]
    ogate = row_scale * total[:, 2 * LANES : 3 * LANES]
    new_n = keep * small_ref[:seqs, :DK] + write * key_vec
    new_n_ref[...] = new_n
    denominator = jnp.maximum(
        jnp.abs(jnp.sum(query * new_n, axis=1, keepdims=True)), jnp.exp(-new_m)
    )
    columns = jnp.where(lane < DK, query_key, write * query_key).T
    rows = []
    for b in range(seqs):
        query_b = columns[:DK, b : b + 1]
        key_b = columns[DK:, b : b + 1]
        new_c = keep[b : b + 1, :] * c_ref[b] + key_b * value_vec[b : b + 1, :]
        new_c_ref[b] = new_c
        rows.append(jnp.sum(query_b * new_c, axis=0, keepdims=True))
    me = lax.axis_index("kv")
    theirs = parts_ref[pl.ds(me + 1 - 2 * lax.rem(me, 2), 1)][0]
    theirs = theirs[:, 3 * LANES :].astype(jnp.float32)
    start, share = LANES // 2, other_ref.shape[1] // seqs
    other_ref[...] = jnp.concatenate(
        [theirs[b : b + 1, start : start + share] for b in range(seqs)], axis=1
    )
    head_out = jnp.concatenate(rows, axis=0) / denominator
    merged = head_out * small_ref[2 * seqs + 1 : 2 * seqs + 2, :] / (1.0 + jnp.exp(-ogate))
    merged = merged.astype(out_ref.dtype)
    for place in range(out_ref.shape[0]):
        out_ref[place] = merged


def cell(parts, state_c, small, width):
    count, seqs, _ = parts.shape
    *states, other, out = pl.pallas_call(
        cell_kernel,
        out_shape=(
            jax.ShapeDtypeStruct((seqs, DK, DV), jnp.float32),
            jax.ShapeDtypeStruct((seqs, DK), jnp.float32),
            jax.ShapeDtypeStruct((1, seqs), jnp.float32),
            jax.ShapeDtypeStruct((1, width), jnp.float32),
            jax.ShapeDtypeStruct((count, seqs, DV), jnp.bfloat16),
        ),
        in_specs=[VMEM] * 3,
        out_specs=(VMEM,) * 5,
        compiler_params=SMALL,
        name="cell",
    )(
        parts, state_c.reshape(seqs, DK, DV), small,
    )
    return states, other, out


def residual_kernel(parts_ref, tokens_ref, own_ref, out_ref):
    total = parts_ref[0].astype(jnp.float32)
    for k in range(1, parts_ref.shape[0]):
        total += parts_ref[k].astype(jnp.float32)
    middle = (tokens_ref[...].astype(jnp.float32) + total).astype(own_ref.dtype)
    own_ref[...] = middle
    middle = middle.astype(jnp.float32)
    feats, seqs = middle.shape
    copies = out_ref.shape[0] // 2
    for half in range(2):
        at = half * (seqs // 2)
        picked = middle[:, at : at + seqs // 2]
        packed = jnp.concatenate([picked[: feats // 2], picked[feats // 2 :]], axis=1)
        packed = packed.astype(out_ref.dtype)
        for copy in range(copies):
            out_ref[half * copies + copy] = packed


def residual(parts, tokens):
    count, feats, seqs = parts.shape
    return pl.pallas_call(
        residual_kernel,
        out_shape=(
            jax.ShapeDtypeStruct((feats, seqs), parts.dtype),
            jax.ShapeDtypeStruct((2 * count, feats // 2, seqs), parts.dtype),
        ),
        in_specs=[VMEM, VMEM],
        out_specs=(VMEM, VMEM),
        compiler_params=SMALL,
        name="residual",
    )(parts, tokens)


def finish_kernel(parts_ref, middle_ref, *refs):
    count = (len(refs) - 3) // 2
    states, out_ref, targets = refs[:count], refs[count], refs[count + 1 : -2]
    tokens, sems = refs[-2:]
    copies = [
        pltpu.make_async_copy(state, target, sems.at[k])
        for k, (state, target) in enumerate(zip(states, targets))
    ]
    for copy in copies:
        copy.start()
    total = parts_ref[0].astype(jnp.float32)
    for k in range(1, parts_ref.shape[0]):
        total += parts_ref[k].astype(jnp.float32)
    tokens[...] = (middle_ref[...].astype(jnp.float32) + total).astype(tokens.dtype)
    copies.append(pltpu.make_async_copy(tokens, out_ref, sems.at[count]))
    copies[count].start()
    for copy in copies:
        copy.wait()


def finish(parts, middle, *states):
    return pl.pallas_call(
        finish_kernel,
        out_shape=(
            jax.ShapeDtypeStruct(parts.shape[1:], parts.dtype),
            *(jax.ShapeDtypeStruct(one.shape, one.dtype) for one in states),
        ),
        in_specs=[VMEM] * (2 + len(states)),
        out_specs=(ANY,) * (1 + len(states)),
        scratch_shapes=[
            pltpu.VMEM(parts.shape[1:], parts.dtype),
            pltpu.SemaphoreType.DMA((1 + len(states),)),
        ],
        compiler_params=SMALL,
        name="finish",
    )(parts, middle, *states)


def pack_kernel(gate_ref, up_ref, out_ref, sems):
    units = gate_ref.shape[0]
    copies = [
        pltpu.make_async_copy(source, out_ref.at[pl.ds(k * units, units)], sems.at[k])
        for k, source in enumerate((gate_ref, up_ref))
    ]
    for copy in copies:
        copy.start()
    for copy in copies:
        copy.wait()


def pack(gate, up):
    units, rows = gate.shape
    return pl.pallas_call(
        pack_kernel,
        out_shape=jax.ShapeDtypeStruct((2 * units, rows), gate.dtype),
        in_specs=[ANY, ANY],
        out_specs=VMEM,
        scratch_shapes=[pltpu.SemaphoreType.DMA((2,))],
        compiler_params=SMALL,
        name="pack",
    )(gate, up)


def widen_kernel(x_ref, vectors_ref, gain_ref, own_ref, other_ref, out_ref):
    blocks = x_ref.shape[0] // 2
    half = x_ref.shape[2] // 2
    units = own_ref.shape[0]
    cols = out_ref.shape[1]
    last = cols - LANES
    place = lax.rem(lax.axis_index("kv"), 2)

    def features(which):
        packed = x_ref[pl.ds(which * blocks, blocks)].astype(jnp.float32)
        both = jnp.concatenate([packed[:, :, :half], packed[:, :, half:]], axis=1)
        return both.reshape(-1, half).T

    own, other = features(place), features(1 - place)
    squares = jnp.sum(own * own, axis=1, keepdims=True) + jnp.sum(
        other * other, axis=1, keepdims=True
    )
    own = (own * vectors_ref[3:4, :]).astype(jnp.bfloat16)
    other = (other * gain_ref[...]).astype(jnp.bfloat16)
    out_ref[:, :last] = (
        transposed_product(own, own_ref[:last, :]) + transposed_product(other, other_ref[:last, :])
    ).astype(out_ref.dtype)
    filler = jnp.zeros((cols - units, own_ref.shape[1]), own_ref.dtype)
    rest = transposed_product(
        own, jnp.concatenate([own_ref[last:, :], filler], axis=0)
    ) + transposed_product(other, jnp.concatenate([other_ref[last:, :], filler], axis=0))
    lane = lax.broadcasted_iota(jnp.int32, rest.shape, 1)
    out_ref[:, last:] = jnp.where(lane == units - last, squares, rest).astype(out_ref.dtype)


def widen(x, vectors, other_gain, own, other):
    cols = (own.shape[0] // LANES + 1) * LANES
    return pl.pallas_call(
        widen_kernel,
        out_shape=jax.ShapeDtypeStruct((x.shape[2] // 2, cols), jnp.bfloat16),
        in_specs=[VMEM] * 5,
        out_specs=VMEM,
        compiler_params=SMALL,
        name="widen",
    )(x, vectors, other_gain, own, other)


def body(
    tokens,
    norm_gain,
    w_query,
    w_key,
    w_value,
    w_ogate,
    w_igate,
    w_fgate,
    igate_bias,
    fgate_bias,
    state_c,
    state_n,
    state_m,
    head_gain,
    w_out,
    ffn_gain,
    w_gate,
    w_up,
    w_down,
):
    n_kv, n_tp = lax.axis_size("kv"), lax.axis_size("tp")
    seqs, feats = tokens.shape
    units = w_gate.shape[1]
    rows = n_tp * feats
    own_seqs = seqs // n_kv

    wide = [norm_gain[None], w_igate.T, w_fgate.T, ffn_gain[None]]
    vectors = jnp.concatenate(wide, axis=0).astype(jnp.float32)
    narrow = [
        state_n.reshape(own_seqs, DK), state_m.T, head_gain.astype(jnp.float32),
        jnp.stack([igate_bias, fgate_bias], axis=1),
    ]
    narrow = [jnp.pad(one, ((0, 0), (0, LANES - one.shape[1]))) for one in narrow]
    share = rows // own_seqs
    gain_tile = jnp.pad(
        ffn_gain.astype(jnp.float32).reshape(own_seqs, share),
        ((0, 0), (LANES // 2, LANES // 2 - share)),
    )
    small = jnp.concatenate([narrow[0], gain_tile, *narrow[1:]], axis=0)
    token_copies, own_tokens = spread(tokens.T, n_tp)
    token_rows = exchanged(token_copies, "tp").reshape(rows, seqs)
    w_both = jnp.concatenate([w_query.T, w_key.T], axis=0)
    parts, small = project(token_rows, vectors, small, w_both, w_value, w_ogate)
    arrived = exchanged(parts.reshape(n_kv, own_seqs, -1), "kv")
    states, other_gain, merged = cell(arrived, state_c, small, rows)
    merged, gate, up = lax.optimization_barrier((merged, w_gate.T, w_up.T))
    own_weights = pack(gate, up)
    merged_all = exchanged(merged, "kv").reshape(seqs, -1)
    swap = [(k, k + 1 - 2 * (k % 2)) for k in range(n_kv)]
    other_weights = lax.ppermute(own_weights, "kv", swap)
    attn_part = jnp.dot(merged_all, w_out, preferred_element_type=jnp.float32)
    attn_part = attn_part.astype(jnp.bfloat16).T.reshape(n_tp, feats, seqs)
    own_middle, middle_copies = residual(exchanged(attn_part, "tp"), own_tokens)
    pairs = [[k * n_tp + t for t in range(2 * n_tp)] for k in range(0, n_kv, 2)]
    middle_rows = exchanged(middle_copies, ("kv", "tp"), pairs)
    partial = widen(middle_rows, vectors, other_gain, own_weights, other_weights)
    halves = [list(range(place, n_kv, 2)) for place in range(2)]
    arrived = exchanged(partial.reshape(n_kv // 2, own_seqs, -1), "kv", halves)
    sums = arrived.astype(jnp.float32).sum(axis=0)
    gate_sum, up_sum, total = sums[:, :units], sums[:, units : 2 * units], sums[:, 2 * units]
    ffn_scale = lax.rsqrt(total / D + norm_eps)[:, None]
    hidden = (jax.nn.silu(ffn_scale * gate_sum) * (ffn_scale * up_sum)).astype(jnp.bfloat16)
    hidden_all = exchanged(
        jnp.broadcast_to(hidden[None], (n_kv, *hidden.shape)), "kv", [halves[0] + halves[1]]
    ).reshape(seqs, units)
    down_part = jnp.dot(hidden_all, w_down, preferred_element_type=jnp.float32)
    down_part = down_part.astype(jnp.bfloat16).T.reshape(n_tp, feats, seqs)
    out_tokens, new_c, new_n, new_m = finish(
        exchanged(down_part, "tp"), own_middle, *states
    )
    new_n = new_n.reshape(own_seqs, 1, DK)
    return (out_tokens.T, new_c.reshape(state_c.shape), new_n, new_m.T)


def solution(mesh):
    placed = (
        P("grp", ("kv", "tp")),
        P("kv"),
        P("kv", "tp"),
        P("kv", "tp"),
        P("kv", "tp"),
        P("kv", "tp"),
        P("kv", "tp"),
        P("kv", "tp"),
        P("tp"),
        P("tp"),
        P(("grp", "kv"), "tp", None, None),
        P(("grp", "kv"), "tp", None),
        P(("grp", "kv"), "tp"),
        P("tp", None),
        P("tp", "kv"),
        P("kv"),
        P("kv", "tp"),
        P("kv", "tp"),
        P("tp", "kv"),
    )
    return jax.shard_map(
        body,
        mesh=mesh,
        in_specs=placed,
        out_specs=(
            P("grp", ("kv", "tp")),
            P(("grp", "kv"), "tp", None, None),
            P(("grp", "kv"), "tp", None),
            P(("grp", "kv"), "tp"),
        ),
        check_vma=False,
    )
```

```python
import jax
import jax.numpy as jnp
from jax import lax
from jax.experimental import pallas as pl
from jax.experimental.pallas import tpu as pltpu
from jax.sharding import PartitionSpec as P


D = 4096
DK = 64
DV = 128
LANES = 128


norm_eps = 1e-06
igate_cap = 1.5

VMEM = pl.BlockSpec(memory_space=pltpu.VMEM)
ANY = pl.BlockSpec(memory_space=pl.ANY)
SMALL = pltpu.CompilerParams(vmem_limit_bytes=8 * 2**20)


def exchanged(blocks, axis, groups=None):
    return lax.all_to_all(
        blocks, axis, split_axis=0, concat_axis=0, tiled=True, axis_index_groups=groups
    )


def spread_kernel(value_ref, out_ref, own_ref):
    value = value_ref[...]
    own_ref[...] = value
    for copy in range(out_ref.shape[0]):
        out_ref[copy] = value


def spread(value, count):
    return pl.pallas_call(
        spread_kernel,
        out_shape=(
            jax.ShapeDtypeStruct((count, *value.shape), value.dtype),
            jax.ShapeDtypeStruct(value.shape, value.dtype),
        ),
        in_specs=[VMEM],
        out_specs=(VMEM, VMEM),
        compiler_params=SMALL,
        name="spread",
    )(value)


def transposed_product(x, weight):
    return lax.dot_general(
        x, weight, (((1,), (1,)), ((), ())), preferred_element_type=jnp.float32
    )


def project_kernel(
    x_ref, vectors_ref, small_ref, both_ref, value_ref, ogate_ref, out_ref, handed_ref
):
    handed_ref[...] = small_ref[...]
    x = x_ref[...].astype(jnp.float32).T
    normed = (x * vectors_ref[0:1, :]).astype(jnp.bfloat16)
    out_ref[:, :LANES] = transposed_product(normed, both_ref[...]).astype(out_ref.dtype)
    out_ref[:, LANES : 2 * LANES] = jnp.dot(
        normed, value_ref[...], preferred_element_type=jnp.float32
    ).astype(out_ref.dtype)
    out_ref[:, 2 * LANES : 3 * LANES] = jnp.dot(
        normed, ogate_ref[...], preferred_element_type=jnp.float32
    ).astype(out_ref.dtype)
    wide = normed.astype(jnp.float32)
    squares = jnp.sum(x * x, axis=1, keepdims=True)
    igate = jnp.sum(wide * vectors_ref[1:2, :], axis=1, keepdims=True)
    fgate = jnp.sum(wide * vectors_ref[2:3, :], axis=1, keepdims=True)
    lane = lax.broadcasted_iota(jnp.int32, (x.shape[0], LANES), 1)
    tail = jnp.where(
        lane == 0, igate, jnp.where(lane == 1, fgate, jnp.where(lane == 2, squares, 0.0))
    )
    own = (small_ref.shape[0] - 3) // 2
    gain_tile = small_ref[own : 2 * own, :]
    tail += jnp.concatenate([gain_tile] * (x.shape[0] // own), axis=0)
    out_ref[:, 3 * LANES :] = tail.astype(out_ref.dtype)


def project(x, vectors, small, w_both, w_value, w_ogate):
    return pl.pallas_call(
        project_kernel,
        out_shape=(
            jax.ShapeDtypeStruct((x.shape[1], 4 * LANES), jnp.bfloat16),
            jax.ShapeDtypeStruct(small.shape, small.dtype),
        ),
        in_specs=[VMEM] * 6,
        out_specs=(VMEM, VMEM),
        compiler_params=SMALL,
        name="project",
    )(x, vectors, small, w_both, w_value, w_ogate)


def cell_kernel(
    parts_ref, c_ref, small_ref,
    new_c_ref, new_n_ref, new_m_ref, other_ref, out_ref,
):
    total = parts_ref[0].astype(jnp.float32)
    for k in range(1, parts_ref.shape[0]):
        total += parts_ref[k].astype(jnp.float32)
    seqs = total.shape[0]
    tail = total[:, 3 * LANES :]
    row_scale = lax.rsqrt(tail[:, 2:3] / D + norm_eps)
    igate = igate_cap * jnp.tanh((row_scale * tail[:, 0:1] + small_ref[2 * seqs + 2 : 2 * seqs + 3, 0:1]) / igate_cap)
    fgate = row_scale * tail[:, 1:2] + small_ref[2 * seqs + 2 : 2 * seqs + 3, 1:2]
    diagonal = lax.broadcasted_iota(jnp.int32, (seqs, seqs), 0) == lax.broadcasted_iota(
        jnp.int32, (seqs, seqs), 1
    )
    state_m = jnp.sum(jnp.where(diagonal, small_ref[2 * seqs : 2 * seqs + 1, :seqs], 0.0), axis=1, keepdims=True)
    log_keep = jnp.minimum(fgate, 0.0) - jnp.log1p(jnp.exp(-jnp.abs(fgate)))
    carried = log_keep + state_m
    new_m = jnp.maximum(carried, igate)
    keep = jnp.exp(carried - new_m)
    write = jnp.exp(igate - new_m)
    new_m_ref[...] = jnp.sum(jnp.where(diagonal, new_m, 0.0), axis=0, keepdims=True)
    lane = lax.broadcasted_iota(jnp.int32, (seqs, LANES), 1)
    first = total[:, :LANES]
    query_key = row_scale * jnp.where(lane < DK, first, first * DK ** (-0.5))
    query = query_key[:, :DK]
    key_vec = query_key[:, DK:]
    value_vec = row_scale * total[:, LANES : 2 * LANES]
    ogate = row_scale * total[:, 2 * LANES : 3 * LANES]
    new_n = keep * small_ref[:seqs, :DK] + write * key_vec
    new_n_ref[...] = new_n
    denominator = jnp.maximum(
        jnp.abs(jnp.sum(query * new_n, axis=1, keepdims=True)), jnp.exp(-new_m)
    )
    columns = jnp.where(lane < DK, query_key, write * query_key).T
    rows = []
    for b in range(seqs):
        query_b = columns[:DK, b : b + 1]
        key_b = columns[DK:, b : b + 1]
        new_c = keep[b : b + 1, :] * c_ref[b] + key_b * value_vec[b : b + 1, :]
        new_c_ref[b] = new_c
        rows.append(jnp.sum(query_b * new_c, axis=0, keepdims=True))
    me = lax.axis_index("kv")
    theirs = parts_ref[pl.ds(me + 1 - 2 * lax.rem(me, 2), 1)][0]
    theirs = theirs[:, 3 * LANES :].astype(jnp.float32)
    start, share = LANES // 2, other_ref.shape[1] // seqs
    other_ref[...] = jnp.concatenate(
        [theirs[b : b + 1, start : start + share] for b in range(seqs)], axis=1
    )
    head_out = jnp.concatenate(rows, axis=0) / denominator
    merged = head_out * small_ref[2 * seqs + 1 : 2 * seqs + 2, :] / (1.0 + jnp.exp(-ogate))
    merged = merged.astype(out_ref.dtype)
    for place in range(out_ref.shape[0]):
        out_ref[place] = merged


def cell(parts, state_c, small, width):
    count, seqs, _ = parts.shape
    *states, other, out = pl.pallas_call(
        cell_kernel,
        out_shape=(
            jax.ShapeDtypeStruct((seqs, DK, DV), jnp.float32),
            jax.ShapeDtypeStruct((seqs, DK), jnp.float32),
            jax.ShapeDtypeStruct((1, seqs), jnp.float32),
            jax.ShapeDtypeStruct((1, width), jnp.float32),
            jax.ShapeDtypeStruct((count, seqs, DV), jnp.bfloat16),
        ),
        in_specs=[VMEM] * 3,
        out_specs=(VMEM,) * 5,
        compiler_params=SMALL,
        name="cell",
    )(
        parts, state_c.reshape(seqs, DK, DV), small,
    )
    return states, other, out


def residual_kernel(parts_ref, tokens_ref, own_ref, out_ref):
    total = parts_ref[0].astype(jnp.float32)
    for k in range(1, parts_ref.shape[0]):
        total += parts_ref[k].astype(jnp.float32)
    middle = (tokens_ref[...].astype(jnp.float32) + total).astype(own_ref.dtype)
    own_ref[...] = middle
    middle = middle.astype(jnp.float32)
    feats, seqs = middle.shape
    copies = out_ref.shape[0] // 2
    for half in range(2):
        at = half * (seqs // 2)
        picked = middle[:, at : at + seqs // 2]
        packed = jnp.concatenate([picked[: feats // 2], picked[feats // 2 :]], axis=1)
        packed = packed.astype(out_ref.dtype)
        for copy in range(copies):
            out_ref[half * copies + copy] = packed


def residual(parts, tokens):
    count, feats, seqs = parts.shape
    return pl.pallas_call(
        residual_kernel,
        out_shape=(
            jax.ShapeDtypeStruct((feats, seqs), parts.dtype),
            jax.ShapeDtypeStruct((2 * count, feats // 2, seqs), parts.dtype),
        ),
        in_specs=[VMEM, VMEM],
        out_specs=(VMEM, VMEM),
        compiler_params=SMALL,
        name="residual",
    )(parts, tokens)


def finish_kernel(parts_ref, middle_ref, *refs):
    count = (len(refs) - 3) // 2
    states, out_ref, targets = refs[:count], refs[count], refs[count + 1 : -2]
    tokens, sems = refs[-2:]
    copies = [
        pltpu.make_async_copy(state, target, sems.at[k])
        for k, (state, target) in enumerate(zip(states, targets))
    ]
    for copy in copies:
        copy.start()
    blocks, half = parts_ref.shape[0] // 2, parts_ref.shape[2] // 2
    sums = []
    for place in range(2):
        total = parts_ref[place * blocks].astype(jnp.float32)
        for k in range(1, blocks):
            total += parts_ref[place * blocks + k].astype(jnp.float32)
        sums.append(total)
    total = jnp.concatenate(
        [
            jnp.concatenate([one[:, :half] for one in sums], axis=1),
            jnp.concatenate([one[:, half:] for one in sums], axis=1),
        ],
        axis=0,
    )
    tokens[...] = (middle_ref[...].astype(jnp.float32) + total).astype(tokens.dtype)
    copies.append(pltpu.make_async_copy(tokens, out_ref, sems.at[count]))
    copies[count].start()
    for copy in copies:
        copy.wait()


def finish(parts, middle, *states):
    return pl.pallas_call(
        finish_kernel,
        out_shape=(
            jax.ShapeDtypeStruct(middle.shape, middle.dtype),
            *(jax.ShapeDtypeStruct(one.shape, one.dtype) for one in states),
        ),
        in_specs=[VMEM] * (2 + len(states)),
        out_specs=(ANY,) * (1 + len(states)),
        scratch_shapes=[
            pltpu.VMEM(middle.shape, middle.dtype),
            pltpu.SemaphoreType.DMA((1 + len(states),)),
        ],
        compiler_params=SMALL,
        name="finish",
    )(parts, middle, *states)


def pack_kernel(*refs):
    sources, out_ref, sems = refs[:-2], refs[-2], refs[-1]
    units = sources[0].shape[0]
    copies = [
        pltpu.make_async_copy(source, out_ref.at[pl.ds(k * units, units)], sems.at[k])
        for k, source in enumerate(sources)
    ]
    for copy in copies:
        copy.start()
    for copy in copies:
        copy.wait()


def pack(*arrays):
    units, rows = arrays[0].shape
    count = len(arrays)
    return pl.pallas_call(
        pack_kernel,
        out_shape=jax.ShapeDtypeStruct((count * units, rows), arrays[0].dtype),
        in_specs=[ANY] * count,
        out_specs=VMEM,
        scratch_shapes=[pltpu.SemaphoreType.DMA((count,))],
        compiler_params=SMALL,
        name="pack",
    )(*arrays)


def lower_kernel(hidden_ref, own_ref, other_ref, out_ref):
    units = hidden_ref.shape[1]
    blocks, feats, _ = out_ref.shape
    blocks //= 2
    place = lax.rem(lax.axis_index("kv"), 2)
    hidden = hidden_ref[...]

    def product(weights_ref):
        down = jnp.dot(
            hidden, weights_ref[2 * units :, :], preferred_element_type=jnp.float32
        ).T.reshape(blocks, 2, feats, hidden.shape[0])
        return jnp.concatenate([down[:, 0], down[:, 1]], axis=2).astype(out_ref.dtype)

    out_ref[pl.ds(place * blocks, blocks)] = product(own_ref)
    out_ref[pl.ds((1 - place) * blocks, blocks)] = product(other_ref)


def lower(hidden, own, other, count, feats):
    return pl.pallas_call(
        lower_kernel,
        out_shape=jax.ShapeDtypeStruct(
            (2 * count, feats // 2, 2 * hidden.shape[0]), jnp.bfloat16
        ),
        in_specs=[VMEM] * 3,
        out_specs=VMEM,
        compiler_params=SMALL,
        name="lower",
    )(hidden, own, other)


def widen_kernel(x_ref, vectors_ref, gain_ref, own_ref, other_ref, out_ref):
    blocks = x_ref.shape[0] // 2
    half = x_ref.shape[2] // 2
    units = own_ref.shape[0] // 3 * 2
    cols = out_ref.shape[1]
    last = cols - LANES
    place = lax.rem(lax.axis_index("kv"), 2)

    def features(which):
        packed = x_ref[pl.ds(which * blocks, blocks)].astype(jnp.float32)
        both = jnp.concatenate([packed[:, :, :half], packed[:, :, half:]], axis=1)
        return both.reshape(-1, half).T

    own, other = features(place), features(1 - place)
    squares = jnp.sum(own * own, axis=1, keepdims=True) + jnp.sum(
        other * other, axis=1, keepdims=True
    )
    own = (own * vectors_ref[3:4, :]).astype(jnp.bfloat16)
    other = (other * gain_ref[...]).astype(jnp.bfloat16)
    out_ref[:, :last] = (
        transposed_product(own, own_ref[:last, :]) + transposed_product(other, other_ref[:last, :])
    ).astype(out_ref.dtype)
    filler = jnp.zeros((cols - units, own_ref.shape[1]), own_ref.dtype)
    rest = transposed_product(
        own, jnp.concatenate([own_ref[last:units, :], filler], axis=0)
    ) + transposed_product(other, jnp.concatenate([other_ref[last:units, :], filler], axis=0))
    lane = lax.broadcasted_iota(jnp.int32, rest.shape, 1)
    out_ref[:, last:] = jnp.where(lane == units - last, squares, rest).astype(out_ref.dtype)


def widen(x, vectors, other_gain, own, other):
    cols = (own.shape[0] // 3 * 2 // LANES + 1) * LANES
    return pl.pallas_call(
        widen_kernel,
        out_shape=jax.ShapeDtypeStruct((x.shape[2] // 2, cols), jnp.bfloat16),
        in_specs=[VMEM] * 5,
        out_specs=VMEM,
        compiler_params=SMALL,
        name="widen",
    )(x, vectors, other_gain, own, other)


def body(
    tokens,
    norm_gain,
    w_query,
    w_key,
    w_value,
    w_ogate,
    w_igate,
    w_fgate,
    igate_bias,
    fgate_bias,
    state_c,
    state_n,
    state_m,
    head_gain,
    w_out,
    ffn_gain,
    w_gate,
    w_up,
    w_down,
):
    n_kv, n_tp = lax.axis_size("kv"), lax.axis_size("tp")
    seqs, feats = tokens.shape
    units = w_gate.shape[1]
    rows = n_tp * feats
    own_seqs = seqs // n_kv

    wide = [norm_gain[None], w_igate.T, w_fgate.T, ffn_gain[None]]
    vectors = jnp.concatenate(wide, axis=0).astype(jnp.float32)
    narrow = [
        state_n.reshape(own_seqs, DK), state_m.T, head_gain.astype(jnp.float32),
        jnp.stack([igate_bias, fgate_bias], axis=1),
    ]
    narrow = [jnp.pad(one, ((0, 0), (0, LANES - one.shape[1]))) for one in narrow]
    share = rows // own_seqs
    gain_tile = jnp.pad(
        ffn_gain.astype(jnp.float32).reshape(own_seqs, share),
        ((0, 0), (LANES // 2, LANES // 2 - share)),
    )
    small = jnp.concatenate([narrow[0], gain_tile, *narrow[1:]], axis=0)
    token_copies, own_tokens = spread(tokens.T, n_tp)
    token_rows = exchanged(token_copies, "tp").reshape(rows, seqs)
    w_both = jnp.concatenate([w_query.T, w_key.T], axis=0)
    parts, small = project(token_rows, vectors, small, w_both, w_value, w_ogate)
    arrived = exchanged(parts.reshape(n_kv, own_seqs, -1), "kv")
    states, other_gain, merged = cell(arrived, state_c, small, rows)
    merged, gate, up, down = lax.optimization_barrier((merged, w_gate.T, w_up.T, w_down))
    swap = [(k, k + 1 - 2 * (k % 2)) for k in range(n_kv)]
    merged_all = exchanged(merged, "kv").reshape(seqs, -1)
    own_weights = pack(gate, up, down)
    other_weights = lax.ppermute(own_weights, "kv", swap)
    attn_part = jnp.dot(merged_all, w_out, preferred_element_type=jnp.float32)
    attn_part = attn_part.astype(jnp.bfloat16).T.reshape(n_tp, feats, seqs)
    own_middle, middle_copies = residual(exchanged(attn_part, "tp"), own_tokens)
    pairs = [[k * n_tp + t for t in range(2 * n_tp)] for k in range(0, n_kv, 2)]
    middle_rows = exchanged(middle_copies, ("kv", "tp"), pairs)
    partial = widen(middle_rows, vectors, other_gain, own_weights, other_weights)
    halves = [list(range(place, n_kv, 2)) for place in range(2)]
    arrived = exchanged(partial.reshape(n_kv // 2, own_seqs, -1), "kv", halves)
    sums = arrived.astype(jnp.float32).sum(axis=0)
    gate_sum, up_sum, total = sums[:, :units], sums[:, units : 2 * units], sums[:, 2 * units]
    ffn_scale = lax.rsqrt(total / D + norm_eps)[:, None]
    hidden = (jax.nn.silu(ffn_scale * gate_sum) * (ffn_scale * up_sum)).astype(jnp.bfloat16)
    hidden_half = exchanged(
        jnp.broadcast_to(hidden[None], (n_kv // 2, *hidden.shape)), "kv", halves
    ).reshape(seqs // 2, units)
    down_part = lower(hidden_half, own_weights, other_weights, n_tp, feats)
    out_tokens, new_c, new_n, new_m = finish(
        exchanged(down_part, ("kv", "tp"), pairs), own_middle, *states
    )
    new_n = new_n.reshape(own_seqs, 1, DK)
    return (out_tokens.T, new_c.reshape(state_c.shape), new_n, new_m.T)


def solution(mesh):
    placed = (
        P("grp", ("kv", "tp")),
        P("kv"),
        P("kv", "tp"),
        P("kv", "tp"),
        P("kv", "tp"),
        P("kv", "tp"),
        P("kv", "tp"),
        P("kv", "tp"),
        P("tp"),
        P("tp"),
        P(("grp", "kv"), "tp", None, None),
        P(("grp", "kv"), "tp", None),
        P(("grp", "kv"), "tp"),
        P("tp", None),
        P("tp", "kv"),
        P("kv"),
        P("kv", "tp"),
        P("kv", "tp"),
        P("tp", "kv"),
    )
    return jax.shard_map(
        body,
        mesh=mesh,
        in_specs=placed,
        out_specs=(
            P("grp", ("kv", "tp")),
            P(("grp", "kv"), "tp", None, None),
            P(("grp", "kv"), "tp", None),
            P(("grp", "kv"), "tp"),
        ),
        check_vma=False,
    )
```

```python
import functools

import jax
import jax.numpy as jnp
from jax import lax
from jax.experimental import pallas as pl
from jax.experimental.pallas import tpu as pltpu
from jax.sharding import PartitionSpec as P

D = 4096
DK = 64
DV = 128
LANES = 128


norm_eps = 1e-06
igate_cap = 1.5

VMEM = pl.BlockSpec(memory_space=pltpu.VMEM)
ANY = pl.BlockSpec(memory_space=pl.ANY)
SMALL = pltpu.CompilerParams(vmem_limit_bytes=8 * 2**20)


def exchanged(blocks, axis, groups=None):
    return lax.all_to_all(
        blocks, axis, split_axis=0, concat_axis=0, tiled=True, axis_index_groups=groups
    )


def spread_kernel(value_ref, out_ref, own_ref):
    value = value_ref[...]
    own_ref[...] = value
    for copy in range(out_ref.shape[0]):
        out_ref[copy] = value


def spread(value, count):
    return pl.pallas_call(
        spread_kernel,
        out_shape=(
            jax.ShapeDtypeStruct((count, *value.shape), value.dtype),
            jax.ShapeDtypeStruct(value.shape, value.dtype),
        ),
        in_specs=[VMEM],
        out_specs=(VMEM, VMEM),
        compiler_params=SMALL,
        name="spread",
    )(value)


def transposed_product(x, weight):
    return lax.dot_general(
        x, weight, (((1,), (1,)), ((), ())), preferred_element_type=jnp.float32
    )


def project_kernel(
    x_ref, vectors_ref, small_ref, both_ref, value_ref, ogate_ref, out_ref, handed_ref
):
    handed_ref[...] = small_ref[...]
    x = x_ref[...].astype(jnp.float32).T
    normed = (x * vectors_ref[0:1, :]).astype(jnp.bfloat16)
    out_ref[:, :LANES] = transposed_product(normed, both_ref[...]).astype(out_ref.dtype)
    out_ref[:, LANES : 2 * LANES] = jnp.dot(
        normed, value_ref[...], preferred_element_type=jnp.float32
    ).astype(out_ref.dtype)
    out_ref[:, 2 * LANES : 3 * LANES] = jnp.dot(
        normed, ogate_ref[...], preferred_element_type=jnp.float32
    ).astype(out_ref.dtype)
    wide = normed.astype(jnp.float32)
    squares = jnp.sum(x * x, axis=1, keepdims=True)
    igate = jnp.sum(wide * vectors_ref[1:2, :], axis=1, keepdims=True)
    fgate = jnp.sum(wide * vectors_ref[2:3, :], axis=1, keepdims=True)
    lane = lax.broadcasted_iota(jnp.int32, (x.shape[0], LANES), 1)
    tail = jnp.where(
        lane == 0, igate, jnp.where(lane == 1, fgate, jnp.where(lane == 2, squares, 0.0))
    )
    own = (small_ref.shape[0] - 3) // 2
    gain_tile = small_ref[own : 2 * own, :]
    tail += jnp.concatenate([gain_tile] * (x.shape[0] // own), axis=0)
    out_ref[:, 3 * LANES :] = tail.astype(out_ref.dtype)


def project(x, vectors, small, w_both, w_value, w_ogate):
    return pl.pallas_call(
        project_kernel,
        out_shape=(
            jax.ShapeDtypeStruct((x.shape[1], 4 * LANES), jnp.bfloat16),
            jax.ShapeDtypeStruct(small.shape, small.dtype),
        ),
        in_specs=[VMEM] * 6,
        out_specs=(VMEM, VMEM),
        compiler_params=SMALL,
        name="project",
    )(x, vectors, small, w_both, w_value, w_ogate)


def cell_kernel(
    parts_ref, c_ref, small_ref,
    new_c_ref, new_n_ref, new_m_ref, other_ref, out_ref,
):
    total = parts_ref[0].astype(jnp.float32)
    for k in range(1, parts_ref.shape[0]):
        total += parts_ref[k].astype(jnp.float32)
    seqs = total.shape[0]
    tail = total[:, 3 * LANES :]
    row_scale = lax.rsqrt(tail[:, 2:3] / D + norm_eps)
    igate = igate_cap * jnp.tanh((row_scale * tail[:, 0:1] + small_ref[2 * seqs + 2 : 2 * seqs + 3, 0:1]) / igate_cap)
    fgate = row_scale * tail[:, 1:2] + small_ref[2 * seqs + 2 : 2 * seqs + 3, 1:2]
    diagonal = lax.broadcasted_iota(jnp.int32, (seqs, seqs), 0) == lax.broadcasted_iota(
        jnp.int32, (seqs, seqs), 1
    )
    state_m = jnp.sum(jnp.where(diagonal, small_ref[2 * seqs : 2 * seqs + 1, :seqs], 0.0), axis=1, keepdims=True)
    log_keep = jnp.minimum(fgate, 0.0) - jnp.log1p(jnp.exp(-jnp.abs(fgate)))
    carried = log_keep + state_m
    new_m = jnp.maximum(carried, igate)
    keep = jnp.exp(carried - new_m)
    write = jnp.exp(igate - new_m)
    new_m_ref[...] = jnp.sum(jnp.where(diagonal, new_m, 0.0), axis=0, keepdims=True)
    lane = lax.broadcasted_iota(jnp.int32, (seqs, LANES), 1)
    first = total[:, :LANES]
    query_key = row_scale * jnp.where(lane < DK, first, first * DK ** (-0.5))
    query = query_key[:, :DK]
    key_vec = query_key[:, DK:]
    value_vec = row_scale * total[:, LANES : 2 * LANES]
    ogate = row_scale * total[:, 2 * LANES : 3 * LANES]
    new_n = keep * small_ref[:seqs, :DK] + write * key_vec
    new_n_ref[...] = new_n
    denominator = jnp.maximum(
        jnp.abs(jnp.sum(query * new_n, axis=1, keepdims=True)), jnp.exp(-new_m)
    )
    columns = jnp.where(lane < DK, query_key, write * query_key).T
    rows = []
    for b in range(seqs):
        query_b = columns[:DK, b : b + 1]
        key_b = columns[DK:, b : b + 1]
        new_c = keep[b : b + 1, :] * c_ref[b] + key_b * value_vec[b : b + 1, :]
        new_c_ref[b] = new_c
        rows.append(jnp.sum(query_b * new_c, axis=0, keepdims=True))
    me = lax.axis_index("kv")
    theirs = parts_ref[pl.ds(me + 1 - 2 * lax.rem(me, 2), 1)][0]
    theirs = theirs[:, 3 * LANES :].astype(jnp.float32)
    start, share = LANES // 2, other_ref.shape[1] // seqs
    other_ref[...] = jnp.concatenate(
        [theirs[b : b + 1, start : start + share] for b in range(seqs)], axis=1
    )
    head_out = jnp.concatenate(rows, axis=0) / denominator
    merged = head_out * small_ref[2 * seqs + 1 : 2 * seqs + 2, :] / (1.0 + jnp.exp(-ogate))
    merged = merged.astype(out_ref.dtype)
    for place in range(out_ref.shape[0]):
        out_ref[place] = merged


def cell(parts, state_c, small, width):
    count, seqs, _ = parts.shape
    *states, other, out = pl.pallas_call(
        cell_kernel,
        out_shape=(
            jax.ShapeDtypeStruct((seqs, DK, DV), jnp.float32),
            jax.ShapeDtypeStruct((seqs, DK), jnp.float32),
            jax.ShapeDtypeStruct((1, seqs), jnp.float32),
            jax.ShapeDtypeStruct((1, width), jnp.float32),
            jax.ShapeDtypeStruct((count, seqs, DV), jnp.bfloat16),
        ),
        in_specs=[VMEM] * 3,
        out_specs=(VMEM,) * 5,
        compiler_params=SMALL,
        name="cell",
    )(
        parts, state_c.reshape(seqs, DK, DV), small,
    )
    return states, other, out


def residual_kernel(parts_ref, tokens_ref, own_ref, out_ref):
    total = parts_ref[0].astype(jnp.float32)
    for k in range(1, parts_ref.shape[0]):
        total += parts_ref[k].astype(jnp.float32)
    middle = (tokens_ref[...].astype(jnp.float32) + total).astype(own_ref.dtype)
    own_ref[...] = middle
    middle = middle.astype(jnp.float32)
    feats, seqs = middle.shape
    copies = out_ref.shape[0] // 2
    for half in range(2):
        at = half * (seqs // 2)
        picked = middle[:, at : at + seqs // 2]
        packed = jnp.concatenate([picked[: feats // 2], picked[feats // 2 :]], axis=1)
        packed = packed.astype(out_ref.dtype)
        for copy in range(copies):
            out_ref[half * copies + copy] = packed


def residual(parts, tokens):
    count, feats, seqs = parts.shape
    return pl.pallas_call(
        residual_kernel,
        out_shape=(
            jax.ShapeDtypeStruct((feats, seqs), parts.dtype),
            jax.ShapeDtypeStruct((2 * count, feats // 2, seqs), parts.dtype),
        ),
        in_specs=[VMEM, VMEM],
        out_specs=(VMEM, VMEM),
        compiler_params=SMALL,
        name="residual",
    )(parts, tokens)


def finish_kernel(parts_ref, middle_ref, *refs):
    count = (len(refs) - 3) // 2
    states, out_ref, targets = refs[:count], refs[count], refs[count + 1 : -2]
    tokens, sems = refs[-2:]
    copies = [
        pltpu.make_async_copy(state, target, sems.at[k])
        for k, (state, target) in enumerate(zip(states, targets))
    ]
    for copy in copies:
        copy.start()
    blocks, half = parts_ref.shape[0] // 2, parts_ref.shape[2] // 2
    sums = []
    for place in range(2):
        total = parts_ref[place * blocks].astype(jnp.float32)
        for k in range(1, blocks):
            total += parts_ref[place * blocks + k].astype(jnp.float32)
        sums.append(total)
    total = jnp.concatenate(
        [
            jnp.concatenate([one[:, :half] for one in sums], axis=1),
            jnp.concatenate([one[:, half:] for one in sums], axis=1),
        ],
        axis=0,
    )
    tokens[...] = (middle_ref[...].astype(jnp.float32) + total).astype(tokens.dtype)
    copies.append(pltpu.make_async_copy(tokens, out_ref, sems.at[count]))
    copies[count].start()
    for copy in copies:
        copy.wait()


def finish(parts, middle, *states):
    return pl.pallas_call(
        finish_kernel,
        out_shape=(
            jax.ShapeDtypeStruct(middle.shape, middle.dtype),
            *(jax.ShapeDtypeStruct(one.shape, one.dtype) for one in states),
        ),
        in_specs=[VMEM] * (2 + len(states)),
        out_specs=(ANY,) * (1 + len(states)),
        scratch_shapes=[
            pltpu.VMEM(middle.shape, middle.dtype),
            pltpu.SemaphoreType.DMA((1 + len(states),)),
        ],
        compiler_params=SMALL,
        name="finish",
    )(parts, middle, *states)


def pack_kernel(*refs):
    sources, out_ref, sems = refs[:-2], refs[-2], refs[-1]
    units = sources[0].shape[0]
    copies = [
        pltpu.make_async_copy(source, out_ref.at[pl.ds(k * units, units)], sems.at[k])
        for k, source in enumerate(sources)
    ]
    for copy in copies:
        copy.start()
    for copy in copies:
        copy.wait()


def pack(*arrays):
    units, rows = arrays[0].shape
    count = len(arrays)
    return pl.pallas_call(
        pack_kernel,
        out_shape=jax.ShapeDtypeStruct((count * units, rows), arrays[0].dtype),
        in_specs=[ANY] * count,
        out_specs=VMEM,
        scratch_shapes=[pltpu.SemaphoreType.DMA((count,))],
        compiler_params=SMALL,
        name="pack",
    )(*arrays)


def lower_kernel(hidden_ref, own_ref, other_ref, out_ref):
    units = hidden_ref.shape[1]
    blocks, feats, _ = out_ref.shape
    blocks //= 2
    place = lax.rem(lax.axis_index("kv"), 2)
    hidden = hidden_ref[...]

    def product(weights_ref):
        down = jnp.dot(
            hidden, weights_ref[...], preferred_element_type=jnp.float32
        ).T.reshape(blocks, 2, feats, hidden.shape[0])
        return jnp.concatenate([down[:, 0], down[:, 1]], axis=2).astype(out_ref.dtype)

    out_ref[pl.ds(place * blocks, blocks)] = product(own_ref)
    out_ref[pl.ds((1 - place) * blocks, blocks)] = product(other_ref)


def lower(hidden, own, other, count, feats):
    return pl.pallas_call(
        lower_kernel,
        out_shape=jax.ShapeDtypeStruct(
            (2 * count, feats // 2, 2 * hidden.shape[0]), jnp.bfloat16
        ),
        in_specs=[VMEM] * 3,
        out_specs=VMEM,
        compiler_params=SMALL,
        name="lower",
    )(hidden, own, other)


def widen_kernel(x_ref, vectors_ref, gain_ref, own_ref, other_ref, out_ref):
    blocks = x_ref.shape[0] // 2
    half = x_ref.shape[2] // 2
    units = own_ref.shape[0]
    cols = out_ref.shape[1]
    last = cols - LANES
    place = lax.rem(lax.axis_index("kv"), 2)

    def features(which):
        packed = x_ref[pl.ds(which * blocks, blocks)].astype(jnp.float32)
        both = jnp.concatenate([packed[:, :, :half], packed[:, :, half:]], axis=1)
        return both.reshape(-1, half).T

    own, other = features(place), features(1 - place)
    squares = jnp.sum(own * own, axis=1, keepdims=True) + jnp.sum(
        other * other, axis=1, keepdims=True
    )
    own = (own * vectors_ref[3:4, :]).astype(jnp.bfloat16)
    other = (other * gain_ref[...]).astype(jnp.bfloat16)
    out_ref[:, :last] = (
        transposed_product(own, own_ref[:last, :]) + transposed_product(other, other_ref[:last, :])
    ).astype(out_ref.dtype)
    filler = jnp.zeros((cols - units, own_ref.shape[1]), own_ref.dtype)
    rest = transposed_product(
        own, jnp.concatenate([own_ref[last:units, :], filler], axis=0)
    ) + transposed_product(other, jnp.concatenate([other_ref[last:units, :], filler], axis=0))
    lane = lax.broadcasted_iota(jnp.int32, rest.shape, 1)
    out_ref[:, last:] = jnp.where(lane == units - last, squares, rest).astype(out_ref.dtype)


def widen(x, vectors, other_gain, own, other):
    cols = (own.shape[0] // LANES + 1) * LANES
    return pl.pallas_call(
        widen_kernel,
        out_shape=jax.ShapeDtypeStruct((x.shape[2] // 2, cols), jnp.bfloat16),
        in_specs=[VMEM] * 5,
        out_specs=VMEM,
        compiler_params=SMALL,
        name="widen",
    )(x, vectors, other_gain, own, other)


def body(
    tokens,
    norm_gain,
    w_query,
    w_key,
    w_value,
    w_ogate,
    w_igate,
    w_fgate,
    igate_bias,
    fgate_bias,
    state_c,
    state_n,
    state_m,
    head_gain,
    w_out,
    ffn_gain,
    w_gate,
    w_up,
    w_down,
):
    n_kv, n_tp = lax.axis_size("kv"), lax.axis_size("tp")
    seqs, feats = tokens.shape
    units = w_gate.shape[1]
    rows = n_tp * feats
    own_seqs = seqs // n_kv

    wide = [norm_gain[None], w_igate.T, w_fgate.T, ffn_gain[None]]
    vectors = jnp.concatenate(wide, axis=0).astype(jnp.float32)
    narrow = [
        state_n.reshape(own_seqs, DK), state_m.T, head_gain.astype(jnp.float32),
        jnp.stack([igate_bias, fgate_bias], axis=1),
    ]
    narrow = [jnp.pad(one, ((0, 0), (0, LANES - one.shape[1]))) for one in narrow]
    share = rows // own_seqs
    gain_tile = jnp.pad(
        ffn_gain.astype(jnp.float32).reshape(own_seqs, share),
        ((0, 0), (LANES // 2, LANES // 2 - share)),
    )
    small = jnp.concatenate([narrow[0], gain_tile, *narrow[1:]], axis=0)
    token_copies, own_tokens = spread(tokens.T, n_tp)
    token_rows = exchanged(token_copies, "tp").reshape(rows, seqs)
    w_both = jnp.concatenate([w_query.T, w_key.T], axis=0)
    parts, small = project(token_rows, vectors, small, w_both, w_value, w_ogate)
    arrived = exchanged(parts.reshape(n_kv, own_seqs, -1), "kv")
    states, other_gain, merged = cell(arrived, state_c, small, rows)
    merged, gate, up, down = lax.optimization_barrier((merged, w_gate.T, w_up.T, w_down))
    own_weights = pack(gate, up)
    merged_all = exchanged(merged, "kv").reshape(seqs, -1)
    swap = [(k, k + 1 - 2 * (k % 2)) for k in range(n_kv)]
    other_weights = lax.ppermute(own_weights, "kv", swap)
    other_down = lax.ppermute(down, "kv", swap)
    attn_part = jnp.dot(merged_all, w_out, preferred_element_type=jnp.float32)
    attn_part = attn_part.astype(jnp.bfloat16).T.reshape(n_tp, feats, seqs)
    own_middle, middle_copies = residual(exchanged(attn_part, "tp"), own_tokens)
    pairs = [[k * n_tp + t for t in range(2 * n_tp)] for k in range(0, n_kv, 2)]
    middle_rows = exchanged(middle_copies, ("kv", "tp"), pairs)
    middle_rows, other_down = lax.optimization_barrier((middle_rows, other_down))
    partial = widen(middle_rows, vectors, other_gain, own_weights, other_weights)
    halves = [list(range(place, n_kv, 2)) for place in range(2)]
    arrived = exchanged(partial.reshape(n_kv // 2, own_seqs, -1), "kv", halves)
    sums = arrived.astype(jnp.float32).sum(axis=0)
    gate_sum, up_sum, total = sums[:, :units], sums[:, units : 2 * units], sums[:, 2 * units]
    ffn_scale = lax.rsqrt(total / D + norm_eps)[:, None]
    hidden = (jax.nn.silu(ffn_scale * gate_sum) * (ffn_scale * up_sum)).astype(jnp.bfloat16)
    hidden_half = exchanged(
        jnp.broadcast_to(hidden[None], (n_kv // 2, *hidden.shape)), "kv", halves
    ).reshape(seqs // 2, units)
    down_part = lower(hidden_half, w_down, other_down, n_tp, feats)
    out_tokens, new_c, new_n, new_m = finish(
        exchanged(down_part, ("kv", "tp"), pairs), own_middle, *states
    )
    new_n = new_n.reshape(own_seqs, 1, DK)
    return (out_tokens.T, new_c.reshape(state_c.shape), new_n, new_m.T)


def solution(mesh):
    placed = (
        P("grp", ("kv", "tp")),
        P("kv"),
        P("kv", "tp"),
        P("kv", "tp"),
        P("kv", "tp"),
        P("kv", "tp"),
        P("kv", "tp"),
        P("kv", "tp"),
        P("tp"),
        P("tp"),
        P(("grp", "kv"), "tp", None, None),
        P(("grp", "kv"), "tp", None),
        P(("grp", "kv"), "tp"),
        P("tp", None),
        P("tp", "kv"),
        P("kv"),
        P("kv", "tp"),
        P("kv", "tp"),
        P("tp", "kv"),
    )
    return jax.shard_map(
        body,
        mesh=mesh,
        in_specs=placed,
        out_specs=(
            P("grp", ("kv", "tp")),
            P(("grp", "kv"), "tp", None, None),
            P(("grp", "kv"), "tp", None),
            P(("grp", "kv"), "tp"),
        ),
        check_vma=False,
    )
```
